256 devices in a mesh: ep: 128 (over z, y, x_hi, core), tp: 2 (over x_lo).
Axes of the slice: x: 4 (x_hi: 2, x_lo: 2; x = x_hi * 2 + x_lo), y: 4, z: 8, core: 2. Of those that a mesh axis runs over, the one named last changes fastest.
Arguments:
- tokens: bfloat16 [1536, 2048], P('ep'), may hold values from -6 to 6
- norm_gain: float32 [2048], replicated, may hold values from 0.1 to 1.9
- w_query: bfloat16 [2048, 768], P(None, 'tp'), may hold values from -0.125 to 0.125
- w_key: bfloat16 [2048, 768], P(None, 'tp'), may hold values from -0.125 to 0.125
- w_value: bfloat16 [2048, 768], P(None, 'tp'), may hold values from -0.125 to 0.125
- w_outgate: bfloat16 [2048, 768], P(None, 'tp'), may hold values from -0.125 to 0.125
- w_input_gate: bfloat16 [2048, 4], replicated, may hold values from -0.125 to 0.125
- w_forget_gate: bfloat16 [2048, 4], replicated, may hold values from -0.125 to 0.125
- forget_bias: float32 [4], replicated, may hold values from -1 to 4
- head_gain: float32 [768], replicated, may hold values from 0.1 to 1.9
- w_output: bfloat16 [768, 2048], P('tp'), may hold values from -0.21875 to 0.21875
- memory: float32 [1536, 4, 192, 192], P('ep', 'tp'), may hold values from -2 to 2
- normalizer: float32 [1536, 4, 192], P('ep', 'tp'), may hold values from -2 to 2
- stabilizer: float32 [1536, 4], P('ep', 'tp'), may hold values from -2 to 2
- ffn_gain: float32 [2048], replicated, may hold values from 0.1 to 1.9
- route_ids: int32 [1536, 4], P('ep'), may hold values from 0 to 127, all different within a row; in each aligned block of 12 rows (0 to 11, 12 to 23, ...) at most 2 rows name the same one
- route_probs: float32 [1536, 4], P('ep'), may hold values from 0.05 to 1
- expert_gate: bfloat16 [128, 2048, 1024], P('ep', None, 'tp'), may hold values from -0.125 to 0.125
- expert_up: bfloat16 [128, 2048, 1024], P('ep', None, 'tp'), may hold values from -0.125 to 0.125
- expert_down: bfloat16 [128, 1024, 2048], P('ep', 'tp'), may hold values from -0.1875 to 0.1875
Outputs:
- next_tokens: bfloat16 [1536, 2048], P('ep')
- new_memory: float32 [1536, 4, 192, 192], P('ep', 'tp')
- new_normalizer: float32 [1536, 4, 192], P('ep', 'tp')
- new_stabilizer: float32 [1536, 4], P('ep', 'tp')
The draws below stay inside these ranges and needn't reach their ends.
Inputs may be any that keep to these rules, and one draw needn't show every extreme that they name: `route_ids`: in each aligned block of 12 rows (the rows of one index of ep), no expert appears more than 2 times among the block's routes, and some expert appears exactly 2 times; the 4 experts of a row are different.
All inputs are finite; a program needn't handle non-finite values.
Results may differ from the reference program's by a relative error of at most 0.015.
Values may be sent and summed in bfloat16 or wider, within the bound.
No kernel may reach another device: no remote copies, remote signals or barrier semaphores. Data moves between devices by JAX's collectives and lax.ppermute only.
A program may use at most 128 MiB of HBM per device.

```python
import math
import jax
import jax.numpy as jnp
import numpy as np
from jax import lax

D = 2048
HEADS = 4
DH = 192
FFE = 1024
TOPK = 4
B_DEV = 12
INNER = 768
EXPERTS = 128
BATCH = 1536
CAP = 2
N_EP = 128
N_TP = 2


def block_levels(stream_key, dims, cuts, smallest, high):
    def one(axis_at, blocks):
        steps = jax.random.uniform(jax.random.fold_in(jax.random.fold_in(stream_key, 6), axis_at), (blocks,), jnp.float32, smallest / len(cuts), high / len(cuts))
        return jnp.repeat(jnp.exp(steps), dims[axis_at] // blocks).reshape((-1,) + (1,) * (len(dims) - axis_at - 1))

    loudness = one(*cuts[0])
    for cut in cuts[1:]:
        loudness = loudness * one(*cut)
    return loudness


def shared_out(key, own, number, rows, number_of, top, reach, slope):
    sequence = jax.random.permutation(key, number_of)
    heavy_load, ordinary = portions_of(number_of, rows * top, reach, slope, True), portions_of(number_of, rows * top, reach, slope, False)
    places = jnp.arange(number_of)

    def named(lengths, rotation):
        used = int((lengths > 0).sum())
        fixed = max(1, used // 4)
        moved = fixed + (places - fixed + rotation * (used - fixed)) % max(1, number_of - fixed)
        return jnp.zeros((number_of,), jnp.int32).at[sequence[jnp.where(places < fixed, places, moved)]].set(jnp.asarray(lengths, jnp.int32))

    lengths = jnp.where(number % 4 == 0, named(heavy_load, number // 4), named(ordinary, number - number // 4 - 1))
    mixed = jax.random.permutation(jax.random.fold_in(own, 3), number_of)
    source_of, taker = mixed[0:number_of // 2 * 2:2], mixed[1:number_of // 2 * 2:2]
    margin = jnp.minimum(lengths[source_of] - 1, reach - lengths[taker]) // 2
    margin = jnp.where((source_of == sequence[0]) | (taker == sequence[0]) | (lengths[taker] == 0), 0, jnp.maximum(margin, 0))
    moved = jax.random.randint(jax.random.fold_in(own, 4), (number_of // 2,), 0, 1 << 20) % (margin + 1)
    lengths = lengths.at[source_of].add(-moved).at[taker].add(moved)
    items = jnp.searchsorted(jnp.cumsum(lengths), jnp.arange(rows * top), side="right").astype(jnp.int32)
    table = items.reshape(top, rows).T
    table = table[jax.random.permutation(jax.random.fold_in(own, 1), rows)]
    rotation = jax.random.randint(jax.random.fold_in(own, 2), (rows, 1), 0, top)
    return jnp.take_along_axis(table, (jnp.arange(top)[None, :] + rotation) % top, axis=1)


def portions_of(number_of, total, reach, skew, full):
    weights = [(1 << 20) // math.isqrt(rank ** skew) + 1 for rank in range(1, number_of + 1)]
    largest = reach if full else min(reach, max(-(-total // number_of), total * weights[0] // sum(weights)))
    least = 1 if total - largest >= number_of - 1 else 0
    holding, spare = [largest] + [least] * (number_of - 1), total - largest - least * (number_of - 1)
    while spare > 0:
        free = [i for i in range(1, number_of) if holding[i] < largest] or [i for i in range(1, number_of) if holding[i] < reach]
        mass, budget = sum([weights[i] for i in free]), spare
        for i in free:
            more = min(reach - holding[i], max(1, budget * weights[i] // mass), spare)
            holding[i] = holding[i] + more
            spare = spare - more
    return np.array(holding)


def gaussian(stream_key, shape, spread, reach, shards=(), kind=jnp.bfloat16):
    factor_of = block_levels(stream_key, shape, shards, -0.22, 0.18) if shards else 1.0
    drawn = jax.random.normal(stream_key, shape, jnp.float32) * spread * factor_of
    return jnp.minimum(jnp.maximum(drawn, -reach), reach).astype(kind)


def setup_inputs(seed: int = 0) -> dict:
    keys = jax.random.split(jax.random.key(seed), 21)
    tokens = gaussian(keys[0], (BATCH, D), 1.0, 6.0, ((0, 128),))
    norm_gain = jnp.clip(1.0 + 0.18 * jax.random.normal(keys[1], (D,), jnp.float32), 0.1, 1.9)
    w_query = gaussian(keys[2], (D, INNER), D ** -0.5, 0.125, ((1, 2),))
    w_key = gaussian(keys[3], (D, INNER), D ** -0.5, 0.125, ((1, 2),))
    w_value = gaussian(keys[4], (D, INNER), D ** -0.5, 0.125, ((1, 2),))
    w_outgate = gaussian(keys[5], (D, INNER), D ** -0.5, 0.125, ((1, 2),))
    w_input_gate = gaussian(keys[6], (D, HEADS), D ** -0.5, 0.125)
    w_forget_gate = gaussian(keys[7], (D, HEADS), D ** -0.5, 0.125)
    forget_bias = jnp.clip(jax.random.uniform(keys[8], (HEADS,), jnp.float32, -1.0, 4.0), -1.0, 4.0)
    head_gain = jnp.clip(1.0 + 0.18 * jax.random.normal(keys[9], (INNER,), jnp.float32), 0.1, 1.9)
    w_output = gaussian(keys[10], (INNER, D), INNER ** -0.5, 0.21875, ((0, 2),))
    memory = gaussian(keys[11], (BATCH, HEADS, DH, DH), 0.3, 2.0, ((0, 128), (1, 2)), jnp.float32)
    normalizer = gaussian(keys[12], (BATCH, HEADS, DH), 0.3, 2.0, ((0, 128), (1, 2)), jnp.float32)
    stabilizer = jnp.clip(jax.random.uniform(keys[13], (BATCH, HEADS), jnp.float32, -2.0, 2.0) * block_levels(keys[13], (BATCH, HEADS), ((0, 128), (1, 2)), -0.4, 0.0), -2.0, 2.0)
    ffn_gain = jnp.clip(1.0 + 0.18 * jax.random.normal(keys[14], (D,), jnp.float32), 0.1, 1.9)
    route_ids_keys = jax.random.split(jax.random.fold_in(keys[15], 1), BATCH // B_DEV)
    route_ids_turns = jax.random.permutation(jax.random.fold_in(keys[15], 3), BATCH // B_DEV)
    route_ids = jax.vmap(lambda own, number: shared_out(jax.random.fold_in(keys[15], 2), own, number, B_DEV, EXPERTS, TOPK, CAP, 2))(route_ids_keys, route_ids_turns).reshape((BATCH, TOPK))
    route_probs = jnp.clip(jnp.exp(math.log(1.0) - 2.9957323 * jax.random.uniform(keys[16], (BATCH, TOPK), jnp.float32) ** block_levels(keys[16], (BATCH, TOPK), ((0, 128),), -0.2, 0.2)), 0.05, 1.0)
    expert_gate = gaussian(keys[17], (EXPERTS, D, FFE), D ** -0.5, 0.125, ((0, 128), (2, 2)))
    expert_up = gaussian(keys[18], (EXPERTS, D, FFE), D ** -0.5, 0.125, ((0, 128), (2, 2)))
    expert_down = gaussian(keys[19], (EXPERTS, FFE, D), FFE ** -0.5, 0.1875, ((0, 128), (1, 2)))
    return {"tokens": tokens, "norm_gain": norm_gain, "w_query": w_query, "w_key": w_key, "w_value": w_value, "w_outgate": w_outgate, "w_input_gate": w_input_gate, "w_forget_gate": w_forget_gate, "forget_bias": forget_bias, "head_gain": head_gain, "w_output": w_output, "memory": memory, "normalizer": normalizer, "stabilizer": stabilizer, "ffn_gain": ffn_gain, "route_ids": route_ids, "route_probs": route_probs, "expert_gate": expert_gate, "expert_up": expert_up, "expert_down": expert_down}


EPS = 1e-06

def rms_scaled(values, scales):
    floats = values.astype(jnp.float32)
    return floats * lax.rsqrt(lax.optimization_barrier(jnp.mean(floats * floats, axis=-1, keepdims=True)) + EPS) * scales.astype(jnp.float32)

def expert_apply(inputs):
    expert_rows, gate_w, up_w, down_w = inputs
    gate_val = jnp.dot(expert_rows, gate_w, preferred_element_type=jnp.float32)
    up_val = jnp.dot(expert_rows, up_w, preferred_element_type=jnp.float32)
    hidden = (jax.nn.silu(gate_val) * up_val).astype(jnp.bfloat16)
    half_width = FFE // N_TP
    summed = jnp.zeros((expert_rows.shape[0], D), jnp.float32)
    for tp_part in range(N_TP):
        partial_value = jnp.dot(hidden[:, tp_part * half_width:(tp_part + 1) * half_width], down_w[tp_part * half_width:(tp_part + 1) * half_width], preferred_element_type=jnp.float32).astype(jnp.bfloat16)
        summed = summed + lax.optimization_barrier(partial_value).astype(jnp.float32)
    return summed.astype(jnp.bfloat16)

def reference(tokens, norm_gain, w_query, w_key, w_value, w_outgate, w_input_gate, w_forget_gate, forget_bias, head_gain, w_output, memory, normalizer, stabilizer, ffn_gain, route_ids, route_probs, expert_gate, expert_up, expert_down):
    highest = lax.Precision.HIGHEST
    batch_rows = tokens.shape[0]
    normed = rms_scaled(tokens, norm_gain).astype(jnp.bfloat16)
    query = jnp.dot(normed, w_query, preferred_element_type=jnp.float32).reshape(batch_rows, HEADS, DH)
    key_vec = (jnp.dot(normed, w_key, preferred_element_type=jnp.float32) * DH ** (-0.5)).reshape(batch_rows, HEADS, DH)
    value_vec = jnp.dot(normed, w_value, preferred_element_type=jnp.float32).reshape(batch_rows, HEADS, DH)
    outgate = jnp.dot(normed, w_outgate, preferred_element_type=jnp.float32)
    input_pre = jnp.dot(normed, w_input_gate, preferred_element_type=jnp.float32)
    log_forget = jax.nn.log_sigmoid(jnp.dot(normed, w_forget_gate, preferred_element_type=jnp.float32) + forget_bias)
    new_stab = jnp.maximum(log_forget + stabilizer, input_pre)
    keep_gate = jnp.exp(log_forget + stabilizer - new_stab)
    write_gate = jnp.exp(input_pre - new_stab)
    new_memory = keep_gate[:, :, None, None] * memory + write_gate[:, :, None, None] * key_vec[:, :, :, None] * value_vec[:, :, None, :]
    new_normalizer = keep_gate[:, :, None] * normalizer + write_gate[:, :, None] * key_vec
    numerator = jnp.einsum('bhd,bhde->bhe', query, new_memory, precision=highest)
    denominator = lax.optimization_barrier(jnp.sum(query * new_normalizer, axis=-1))
    readout = numerator / jnp.maximum(jnp.abs(denominator), jnp.exp(-new_stab))[:, :, None]
    normed_read = readout * lax.rsqrt(lax.optimization_barrier(jnp.mean(readout * readout, axis=-1, keepdims=True)) + EPS) * head_gain.reshape(HEADS, DH)
    gated = (normed_read.reshape(batch_rows, HEADS * DH) * jax.nn.sigmoid(outgate)).astype(jnp.bfloat16)
    local_width = HEADS * DH // N_TP
    mix_sum = jnp.zeros((batch_rows, D), jnp.float32)
    for tp_part in range(N_TP):
        partial_value = jnp.dot(gated[:, tp_part * local_width:(tp_part + 1) * local_width], w_output[tp_part * local_width:(tp_part + 1) * local_width], preferred_element_type=jnp.float32).astype(jnp.bfloat16)
        mix_sum = mix_sum + lax.optimization_barrier(partial_value).astype(jnp.float32)
    mixed = mix_sum.astype(jnp.bfloat16)
    resid = (tokens.astype(jnp.float32) + mixed.astype(jnp.float32)).astype(jnp.bfloat16)
    ffn_in = rms_scaled(resid, ffn_gain).astype(jnp.bfloat16)
    weights = route_probs / lax.optimization_barrier(jnp.sum(route_probs, axis=-1, keepdims=True))
    flat_expert = route_ids.reshape(-1).astype(jnp.int32)
    onehot = (flat_expert[:, None] == jnp.arange(EXPERTS, dtype=jnp.int32)[None, :]).astype(jnp.int32)
    per_block = onehot.reshape(N_EP, B_DEV * TOPK, EXPERTS)
    earlier = jnp.cumsum(per_block, axis=1) - per_block
    slot_rank = lax.optimization_barrier(jnp.sum(earlier * per_block, axis=-1)).reshape(-1)
    route_index = jnp.arange(batch_rows * TOPK, dtype=jnp.int32)
    source = route_index // (B_DEV * TOPK)
    slot_index = (source * CAP + slot_rank).astype(jnp.int32)
    token_of = route_index // TOPK
    buffers = jnp.zeros((EXPERTS, N_EP * CAP, D), jnp.bfloat16).at[flat_expert, slot_index].set(ffn_in[token_of])
    results = lax.map(expert_apply, (buffers, expert_gate, expert_up, expert_down))
    picked = results[flat_expert, slot_index].astype(jnp.float32).reshape(batch_rows, TOPK, D)
    combined = lax.optimization_barrier(jnp.sum(picked * weights[:, :, None], axis=1))
    next_tokens = (resid.astype(jnp.float32) + combined).astype(jnp.bfloat16)
    return (next_tokens, new_memory, new_normalizer, new_stab)
```

```python
import jax
import jax.numpy as jnp
from jax import lax
from jax.sharding import Mesh, PartitionSpec as P

EPS = 1e-06
Z, Y, XH, C, TP = 8, 4, 2, 2, 2
EP = ("z", "y", "xh", "c")
F32, BF16 = jnp.float32, jnp.bfloat16
PAD = 16


def rms_scaled(values, scales):
    floats = values.astype(F32)
    return floats * lax.rsqrt(jnp.mean(floats * floats, axis=-1, keepdims=True) + EPS) * scales


def plane_pairs(dy, dx, back):
    pairs = []
    for y in range(Y):
        for xh in range(XH):
            for t in range(TP):
                src = (y * XH + xh) * TP + t
                dst = (((y + dy) % Y) * XH + (xh ^ dx)) * TP + (t ^ dx)
                pairs.append((dst, src) if back else (src, dst))
    return pairs


STEPS = [(dy, dx) for dy in range(Y) for dx in range(XH)]


def plane_exchange(parts, back):
    out = []
    for (dy, dx), part in zip(STEPS, parts):
        if dy == 0 and dx == 0:
            out.append(part)
        else:
            out.append(lax.ppermute(part, ("y", "xh", "tp"), plane_pairs(dy, dx, back)))
    return out


SWAP = [(0, 1), (1, 0)]


def routing(meta, ids):
    experts = meta[:, :, 0:12].astype(jnp.int32)
    high = meta[:, :, 128:140].astype(F32)
    low = meta[:, :, 256:268].astype(F32)
    hit = (experts[None] == ids[:, None, None, None]).astype(F32)
    any_hit = jnp.sum(hit, axis=2)
    w_high = jnp.sum(hit * high[None], axis=2)
    w_low = jnp.sum(hit * low[None], axis=2)
    rows = any_hit.shape[-1]
    before = (jnp.arange(rows)[:, None] < jnp.arange(rows)[None, :]).astype(F32)
    earlier = jnp.einsum("jzb,bc->jzc", any_hit, before)
    slot = (jnp.round(earlier).astype(jnp.int32)[:, :, None, :] == jnp.arange(2)[None, None, :, None]).astype(F32)
    diag = jnp.eye(Z, dtype=F32)

    def spread(values):
        full = (values[:, :, None, :] * slot)[:, :, :, None, :] * diag[None, :, None, :, None]
        full = jnp.pad(full, ((0, 0),) * 4 + ((0, PAD - rows),))
        return full.reshape(8 * Z * 2, Z * PAD).astype(BF16)

    return spread(any_hit), spread(w_high), spread(w_low)


def local(
    tokens,
    norm_gain,
    w_query,
    w_key,
    w_value,
    w_outgate,
    w_input_gate,
    w_forget_gate,
    forget_bias,
    head_gain,
    w_output,
    memory,
    normalizer,
    stabilizer,
    ffn_gain,
    route_ids,
    route_probs,
    expert_gate,
    expert_up,
    expert_down,
):
    tp_rank = lax.axis_index("tp")
    z, y, xh, c = (lax.axis_index(a) for a in EP)
    dev_rows, width = tokens.shape
    dev_heads = memory.shape[1]
    head_dim = memory.shape[2]
    local_width = dev_heads * head_dim
    normed = rms_scaled(tokens, norm_gain).astype(BF16)
    query = jnp.dot(normed, w_query, preferred_element_type=F32)
    key_raw = jnp.dot(normed, w_key, preferred_element_type=F32)
    value_raw = jnp.dot(normed, w_value, preferred_element_type=F32)
    outgate = jnp.dot(normed, w_outgate, preferred_element_type=F32)
    head_start = tp_rank * dev_heads
    input_cols = lax.dynamic_slice_in_dim(w_input_gate, head_start, dev_heads, 1)
    forget_cols = lax.dynamic_slice_in_dim(w_forget_gate, head_start, dev_heads, 1)
    bias_part = lax.dynamic_slice_in_dim(forget_bias, head_start, dev_heads, 0)
    gain_part = lax.dynamic_slice_in_dim(head_gain, tp_rank * local_width, local_width, 0)
    query = query.reshape(dev_rows, dev_heads, head_dim)
    key_vec = (key_raw * head_dim ** (-0.5)).reshape(dev_rows, dev_heads, head_dim)
    value_vec = value_raw.reshape(dev_rows, dev_heads, head_dim)
    input_pre = jnp.dot(normed, input_cols, preferred_element_type=F32)
    log_forget = jax.nn.log_sigmoid(jnp.dot(normed, forget_cols, preferred_element_type=F32) + bias_part)
    new_stab = jnp.maximum(log_forget + stabilizer, input_pre)
    keep_gate = jnp.exp(log_forget + stabilizer - new_stab)
    write_gate = jnp.exp(input_pre - new_stab)
    new_memory = (
        keep_gate[:, :, None, None] * memory
        + write_gate[:, :, None, None] * key_vec[:, :, :, None] * value_vec[:, :, None, :]
    )
    new_normalizer = keep_gate[:, :, None] * normalizer + write_gate[:, :, None] * key_vec
    numerator = jnp.einsum("bhd,bhde->bhe", query, new_memory)
    denominator = jnp.sum(query * new_normalizer, axis=-1)
    readout = numerator / jnp.maximum(jnp.abs(denominator), jnp.exp(-new_stab))[:, :, None]
    normed_read = (
        readout
        * lax.rsqrt(jnp.mean(readout * readout, axis=-1, keepdims=True) + EPS)
        * gain_part.reshape(dev_heads, head_dim)
    )
    gated = (normed_read.reshape(dev_rows, local_width) * jax.nn.sigmoid(outgate)).astype(BF16)
    partial_value = jnp.dot(gated, w_output, preferred_element_type=F32).astype(BF16)
    other_value = lax.ppermute(partial_value, "tp", SWAP)
    mixed = (partial_value.astype(F32) + other_value.astype(F32)).astype(BF16)
    resid = (tokens.astype(F32) + mixed.astype(F32)).astype(BF16)
    ffn_in = rms_scaled(resid, ffn_gain).astype(BF16)

    weights = route_probs / jnp.sum(route_probs, axis=-1, keepdims=True)
    high = lax.reduce_precision(weights, 8, 7)
    low = lax.reduce_precision(weights - high, 8, 7)

    def lanes(values):
        return jnp.pad(values.T, ((0, 0), (0, 128 - dev_rows)))

    meta = jnp.concatenate([lanes(route_ids.astype(F32)), lanes(high), lanes(low)], axis=1)
    meta = jnp.pad(meta, ((0, 0), (0, width - 3 * 128))).astype(BF16)
    block = jnp.concatenate([ffn_in, meta], axis=0)

    column = lax.all_to_all(jnp.broadcast_to(block[None], (Z, PAD, width)), "z", 0, 0, tiled=True)
    column_other = lax.ppermute(column, "c", SWAP)
    dys = jnp.array([s[0] for s in STEPS], jnp.int32)
    dxs = jnp.array([s[1] for s in STEPS], jnp.int32)
    ids = ((z * Y + (y + dys) % Y) * XH + jnp.bitwise_xor(xh, dxs)) * C + c
    sel_a, high_a, low_a = routing(column[:, 12:16, :], ids)
    sel_b, high_b, low_b = routing(column_other[:, 12:16, :], ids)
    out_a = jnp.dot(sel_a, column.reshape(Z * PAD, width), preferred_element_type=F32).astype(BF16)
    out_b = jnp.dot(sel_b, column_other.reshape(Z * PAD, width), preferred_element_type=F32).astype(BF16)
    sent = jnp.concatenate([out_a.reshape(8, 16, width), out_b.reshape(8, 16, width)], axis=1)
    incoming = plane_exchange([sent[j] for j in range(8)], False)
    rows = jnp.concatenate(incoming, axis=0)

    gate_val = jnp.dot(rows, expert_gate[0], preferred_element_type=F32)
    up_val = jnp.dot(rows, expert_up[0], preferred_element_type=F32)
    hidden = (jax.nn.silu(gate_val) * up_val).astype(BF16)
    partial_out = jnp.dot(hidden, expert_down[0], preferred_element_type=F32).astype(BF16)

    partial_out = partial_out.reshape(8, 32, width)
    back = plane_exchange([partial_out[j] for j in range(8)], True)
    back_a = jnp.concatenate([b[0:16] for b in back], axis=0)
    back_b = jnp.concatenate([b[16:32] for b in back], axis=0)

    def combine(w_high, w_low, values):
        dims = (((0,), (0,)), ((), ()))
        return lax.dot_general(w_high, values, dims, preferred_element_type=F32) + lax.dot_general(
            w_low, values, dims, preferred_element_type=F32
        )

    sum_b = combine(high_b, low_b, back_b).astype(BF16)
    sum_b = lax.ppermute(sum_b, "c", SWAP)
    sums = (combine(high_a, low_a, back_a) + sum_b.astype(F32)).astype(BF16)
    sums = lax.all_to_all(sums.reshape(Z, PAD, width)[:, :12], "z", 0, 0, tiled=True)
    combined = jnp.sum(sums.astype(F32), axis=0)
    combined_other = lax.ppermute(combined.astype(BF16), "tp", SWAP)
    next_tokens = (resid.astype(F32) + (combined + combined_other.astype(F32))).astype(BF16)
    return (next_tokens, new_memory, new_normalizer, new_stab)


def solution(mesh):
    fine = Mesh(mesh.devices.reshape(Z, Y, XH, C, TP), (*EP, "tp"))
    ep = EP
    return jax.shard_map(
        local,
        mesh=fine,
        in_specs=(
            P(ep, None),
            P(),
            P(None, "tp"),
            P(None, "tp"),
            P(None, "tp"),
            P(None, "tp"),
            P(),
            P(),
            P(),
            P(),
            P("tp", None),
            P(ep, "tp", None, None),
            P(ep, "tp", None),
            P(ep, "tp"),
            P(),
            P(ep, None),
            P(ep, None),
            P(ep, None, "tp"),
            P(ep, None, "tp"),
            P(ep, "tp", None),
        ),
        out_specs=(P(ep, None), P(ep, "tp", None, None), P(ep, "tp", None), P(ep, "tp")),
        check_vma=False,
    )
```

```python
import jax
import jax.numpy as jnp
from jax import lax
from jax.experimental import pallas as pl
from jax.experimental.pallas import tpu as pltpu
from jax.sharding import Mesh, PartitionSpec as P

EPS = 1e-06
Z, Y, XH, C, TP = 8, 4, 2, 2, 2
EP = ("z", "y", "xh", "c")
F32, BF16 = jnp.float32, jnp.bfloat16
PAD = 16


def plane_pairs(dy, dx, back):
    pairs = []
    for y in range(Y):
        for xh in range(XH):
            for t in range(TP):
                src = (y * XH + xh) * TP + t
                dst = (((y + dy) % Y) * XH + (xh ^ dx)) * TP + (t ^ dx)
                pairs.append((dst, src) if back else (src, dst))
    return pairs


STEPS = [(dy, dx) for dy in range(Y) for dx in range(XH)]


def plane_exchange(parts, back):
    out = []
    for (dy, dx), part in zip(STEPS, parts):
        if dy == 0 and dx == 0:
            out.append(part)
        else:
            out.append(lax.ppermute(part, ("y", "xh", "tp"), plane_pairs(dy, dx, back)))
    return out


SWAP = [(0, 1), (1, 0)]


def cell_kernel(*refs):
    ins, outs, scr = refs[:14], refs[14:18], refs[18:]
    vm = scr[:14]
    out_v = scr[14:18]
    num_v, in_sem, mem_sem, out_sem = scr[18:]
    mem, mem_v = ins[13], vm[13]
    new_mem_hbm, new_mem_v = outs[1], out_v[1]
    rows = 12
    first = (0, 1, 2, 3, 4, 5, 6, 7, 8, 9, 10, 11)
    copies = {i: pltpu.make_async_copy(ins[i], vm[i], in_sem.at[i]) for i in (*first, 12)}
    mem_copies = [pltpu.make_async_copy(mem.at[b], mem_v.at[b], mem_sem.at[b]) for b in range(rows)]
    for i in first:
        copies[i].start()
    for cp in mem_copies:
        cp.start()
    copies[12].start()
    (tok, gain, stab, nrm, bias, hgain, wig, wfg, wk, wq, wv, wo, wout, _) = vm
    copies[0].wait()
    copies[1].wait()
    x = tok[...].astype(F32)
    normed = (x * lax.rsqrt(jnp.mean(x * x, axis=-1, keepdims=True) + EPS) * gain[...]).astype(BF16)
    for i in range(2, 8):
        copies[i].wait()
    t = lax.axis_index("tp")

    def half(values, size):
        return jnp.where(t == 0, values[:, :size], values[:, size : 2 * size])

    input_pre = half(jnp.dot(normed, wig[...], preferred_element_type=F32), 2)
    forget = half(jnp.dot(normed, wfg[...], preferred_element_type=F32), 2) + half(bias[...], 2)
    log_forget = jnp.minimum(forget, 0.0) - jnp.log1p(jnp.exp(-jnp.abs(forget)))
    carried = log_forget + stab[...]
    new_stab = jnp.maximum(carried, input_pre)
    keep = jnp.exp(carried - new_stab)
    write = jnp.exp(input_pre - new_stab)
    out_v[3][...] = new_stab
    copies[8].wait()
    key = jnp.dot(normed, wk[...], preferred_element_type=F32) * 192 ** (-0.5)
    head = lax.broadcasted_iota(jnp.int32, (rows, 384), 1) >= 192
    wkey = jnp.where(head, write[:, 1:2], write[:, 0:1]) * key

    def turned(values):
        return jnp.transpose(jnp.concatenate([values, jnp.zeros((128 - rows, 384), F32)], axis=0))

    wkey_t = turned(wkey)
    copies[9].wait()
    query = jnp.dot(normed, wq[...], preferred_element_type=F32)
    query_t = turned(query)
    copies[10].wait()
    value = jnp.dot(normed, wv[...], preferred_element_type=F32)
    copies[11].wait()
    outgate = jnp.dot(normed, wo[...], preferred_element_type=F32)
    gains = half(hgain[...], 384)
    cut = lambda v, h: v[:, h * 192 : (h + 1) * 192]
    values = [cut(value, h) for h in range(2)]
    keeps = [jnp.broadcast_to(keep[:, h : h + 1], (rows, 192)) for h in range(2)]
    floors = []
    for h in range(2):
        new_norm = keeps[h] * nrm[:, h, :] + cut(wkey, h)
        out_v[2][:, h, :] = new_norm
        den = jnp.sum(cut(query, h) * new_norm, axis=-1, keepdims=True)
        floors.append(jnp.maximum(jnp.abs(den), jnp.exp(-new_stab[:, h : h + 1])))
    out_copies = []
    for b in range(rows):
        mem_copies[b].wait()
        for h in range(2):
            span = slice(h * 192, (h + 1) * 192)
            updated = keeps[h][b : b + 1] * mem_v[b, h] + wkey_t[span, b : b + 1] * values[h][b : b + 1]
            new_mem_v[b, h] = updated
            num_v[h, b : b + 1, :] = jnp.sum(query_t[span, b : b + 1] * updated, axis=0, keepdims=True)
        cp = pltpu.make_async_copy(new_mem_v.at[b], new_mem_hbm.at[b], mem_sem.at[b])
        cp.start()
        out_copies.append(cp)
    total = None
    copies[12].wait()
    for h in range(2):
        readout = num_v[h] / floors[h]
        scaled = readout * lax.rsqrt(jnp.mean(readout * readout, axis=-1, keepdims=True) + EPS) * cut(gains, h)
        gated = (scaled * jax.nn.sigmoid(cut(outgate, h))).astype(BF16)
        part = jnp.dot(gated, wout[h * 192 : (h + 1) * 192, :], preferred_element_type=F32)
        total = part if total is None else total + part
    out_v[0][...] = total.astype(BF16)
    for i in (0, 2, 3):
        cp = pltpu.make_async_copy(out_v[i], outs[i], out_sem.at[i])
        cp.start()
        out_copies.append(cp)
    for cp in out_copies:
        cp.wait()


def cell(tokens, gain, stab, nrm, bias, hgain, wig, wfg, wk, wq, wv, wo, wout, memory):
    args = (tokens, gain, stab, nrm, bias, hgain, wig, wfg, wk, wq, wv, wo, wout, memory)
    outs = [
        jax.ShapeDtypeStruct((12, 2048), BF16),
        jax.ShapeDtypeStruct(memory.shape, F32),
        jax.ShapeDtypeStruct(nrm.shape, F32),
        jax.ShapeDtypeStruct(stab.shape, F32),
    ]
    scratch = [pltpu.VMEM(a.shape, a.dtype) for a in args] + [pltpu.VMEM(o.shape, o.dtype) for o in outs]
    scratch += [
        pltpu.VMEM((2, 12, 192), F32),
        pltpu.SemaphoreType.DMA((14,)),
        pltpu.SemaphoreType.DMA((12,)),
        pltpu.SemaphoreType.DMA((4,)),
    ]
    return pl.pallas_call(
        cell_kernel,
        out_shape=outs,
        in_specs=[pl.BlockSpec(memory_space=pl.ANY)] * len(args),
        out_specs=[pl.BlockSpec(memory_space=pl.ANY)] * 4,
        scratch_shapes=scratch,
        name="cell",
    )(*args)


def mix_kernel(tok, mine, other, gain, ids, probs, block_out, resid_out, scr):
    mixed = (mine[...].astype(F32) + other[...].astype(F32)).astype(BF16)
    resid = (tok[...].astype(F32) + mixed.astype(F32)).astype(BF16)
    resid_out[...] = resid
    x = resid.astype(F32)
    normed = x * lax.rsqrt(jnp.mean(x * x, axis=-1, keepdims=True) + EPS) * gain[...]
    weights = probs[...] / jnp.sum(probs[...], axis=-1, keepdims=True)
    high = weights.astype(BF16)
    low = (weights - high.astype(F32)).astype(BF16)
    z = lax.axis_index("z")
    lane = lax.broadcasted_iota(jnp.int32, (12, 128), 1)
    row = lax.broadcasted_iota(jnp.int32, (12, 128), 0)
    place = (lane == z * PAD + row).astype(F32).astype(BF16)
    scr[...] = jnp.zeros((PAD, 2048), F32)
    scr[0:12, :] = normed
    for i, v in enumerate(((ids[...] + 1).astype(F32).astype(BF16), high, low)):
        spread = lax.dot_general(v, place, (((0,), (0,)), ((), ())), preferred_element_type=F32)
        scr[12:16, i * 128 : (i + 1) * 128] = spread
    block = scr[...].astype(BF16)
    for j in range(Z):
        block_out[j] = block


def mix(tokens, mine, other, gain, ids, probs):
    return pl.pallas_call(
        mix_kernel,
        out_shape=[jax.ShapeDtypeStruct((Z, PAD, 2048), BF16), jax.ShapeDtypeStruct((12, 2048), BF16)],
        scratch_shapes=[pltpu.VMEM((PAD, 2048), F32)],
        name="mix",
    )(tokens, mine, other, gain, ids, probs)


def pack_kernel(col_a, col_b, *refs):
    sent, weights_out = refs[:8], refs[8]
    z, y, xh, c = (lax.axis_index(a) for a in EP)
    row = lax.broadcasted_iota(jnp.int32, (128, 128), 0)
    lane = lax.broadcasted_iota(jnp.int32, (128, 128), 1)
    dy, dx = row >> 5, (row >> 4) & 1
    expert = ((z * Y + ((y + dy) & 3)) * XH + (xh ^ dx)) * C + c + 1
    expert = expert.astype(F32)
    pick = (
        (lax.broadcasted_iota(jnp.int32, (8, 128), 1) & 15) == lax.broadcasted_iota(jnp.int32, (8, 128), 0) + 12
    ).astype(F32).astype(BF16)
    before = (((row >> 4) == (lane >> 4)) & ((row & 15) < (lane & 15))).astype(F32).astype(BF16)
    same = ((row >> 1) & 7) == (lane >> 4)
    slot = (row & 1).astype(F32)
    for side, col in enumerate((col_a, col_b)):
        experts, high, low = (
            jnp.dot(pick, col[:, i * 128 : (i + 1) * 128], preferred_element_type=F32) for i in range(3)
        )
        hit = jnp.zeros((128, 128), F32)
        w_high = jnp.zeros((128, 128), F32)
        w_low = jnp.zeros((128, 128), F32)
        for k in range(4):
            match = experts[k : k + 1] == expert
            hit = hit + jnp.where(match, 1.0, 0.0)
            w_high = w_high + jnp.where(match, high[k : k + 1], 0.0)
            w_low = w_low + jnp.where(match, low[k : k + 1], 0.0)
        earlier = jnp.dot(hit.astype(BF16), before, preferred_element_type=F32)
        mask = same & (earlier == slot)
        weights_out[side, 0] = jnp.where(mask, w_high, 0.0).astype(BF16)
        weights_out[side, 1] = jnp.where(mask, w_low, 0.0).astype(BF16)
        chosen = jnp.dot(
            jnp.where(mask, hit, 0.0).astype(BF16), col[...], preferred_element_type=F32
        ).astype(BF16)
        for j in range(8):
            sent[j][side * 16 : (side + 1) * 16, :] = chosen[j * 16 : (j + 1) * 16]


def pack(col_a, col_b):
    return pl.pallas_call(
        pack_kernel,
        out_shape=[jax.ShapeDtypeStruct((32, 2048), BF16)] * 8 + [jax.ShapeDtypeStruct((2, 2, 128, 128), BF16)],
        name="pack",
    )(col_a, col_b)


def combine_kernel(weights, *refs):
    back, (sum_a, sum_b), scr = refs[:8], refs[8:10], refs[10]
    for side, out in ((1, sum_b), (0, sum_a)):
        for j in range(8):
            scr[side, j * 16 : (j + 1) * 16, :] = back[j][side * 16 : (side + 1) * 16, :]
        dims = (((0,), (0,)), ((), ()))
        values = scr[side]
        total = lax.dot_general(weights[side, 0], values, dims, preferred_element_type=F32)
        total = total + lax.dot_general(weights[side, 1], values, dims, preferred_element_type=F32)
        out[...] = total.astype(out.dtype)


def combine(weights, back):
    return pl.pallas_call(
        combine_kernel,
        out_shape=[jax.ShapeDtypeStruct((128, 2048), F32), jax.ShapeDtypeStruct((128, 2048), BF16)],
        scratch_shapes=[pltpu.VMEM((2, 128, 2048), BF16)],
        name="combine",
    )(weights, *back)


def expert_kernel(*refs):
    rows, (gate, up, down), outs = refs[:8], refs[8:11], refs[11:19]
    x, acc = refs[19:]
    step = pl.program_id(0)

    @pl.when(step == 0)
    def _():
        for j in range(8):
            x[j * 32 : (j + 1) * 32, :] = rows[j][...]
        acc[...] = jnp.zeros_like(acc)

    gate_val = jnp.dot(x[...], gate[0], preferred_element_type=F32)
    up_val = jnp.dot(x[...], up[0], preferred_element_type=F32)
    hidden = (gate_val * jax.nn.sigmoid(gate_val) * up_val).astype(BF16)
    acc[...] += jnp.dot(hidden, down[0], preferred_element_type=F32)

    @pl.when(step == pl.num_programs(0) - 1)
    def _():
        for j in range(8):
            outs[j][...] = acc[j * 32 : (j + 1) * 32, :].astype(BF16)


def expert(rows, gate, up, down):
    chunk, width = 256, 2048
    piece = pl.BlockSpec((32, width), lambda i: (0, 0))
    return pl.pallas_call(
        expert_kernel,
        grid=(gate.shape[2] // chunk,),
        out_shape=[jax.ShapeDtypeStruct((32, width), BF16)] * 8,
        in_specs=[piece] * 8
        + [
            pl.BlockSpec((1, width, chunk), lambda i: (0, 0, i)),
            pl.BlockSpec((1, width, chunk), lambda i: (0, 0, i)),
            pl.BlockSpec((1, chunk, width), lambda i: (0, i, 0)),
        ],
        out_specs=[piece] * 8,
        scratch_shapes=[pltpu.VMEM((256, width), BF16), pltpu.VMEM((256, width), F32)],
        name="expert",
    )(*rows, gate, up, down)


def local(
    tokens,
    norm_gain,
    w_query,
    w_key,
    w_value,
    w_outgate,
    w_input_gate,
    w_forget_gate,
    forget_bias,
    head_gain,
    w_output,
    memory,
    normalizer,
    stabilizer,
    ffn_gain,
    route_ids,
    route_probs,
    expert_gate,
    expert_up,
    expert_down,
):
    partial_value, new_memory, new_normalizer, new_stab = cell(
        tokens,
        norm_gain.reshape(1, -1),
        stabilizer,
        normalizer,
        forget_bias.reshape(1, -1),
        head_gain.reshape(1, -1),
        w_input_gate,
        w_forget_gate,
        w_key,
        w_query,
        w_value,
        w_outgate,
        w_output,
        memory,
    )
    other_value = lax.ppermute(partial_value, "tp", SWAP)
    blocks, resid = mix(tokens, partial_value, other_value, ffn_gain.reshape(1, -1), route_ids, route_probs)
    column = lax.all_to_all(blocks, "z", 0, 0, tiled=True).reshape(Z * PAD, -1)
    column_other = lax.ppermute(column, "c", SWAP)
    *sent, weights = pack(column, column_other)
    incoming = plane_exchange(sent, False)
    outgoing = expert(incoming, expert_gate, expert_up, expert_down)
    back = plane_exchange(outgoing, True)
    sum_a, sum_b = combine(weights, back)
    sum_b = lax.ppermute(sum_b, "c", SWAP)
    sums = (sum_a + sum_b.astype(F32)).astype(BF16).reshape(Z, PAD, -1)
    sums = lax.all_to_all(sums, "z", 0, 0, tiled=True)[:, :12]
    combined = jnp.sum(sums.astype(F32), axis=0)
    combined_other = lax.ppermute(combined.astype(BF16), "tp", SWAP)
    next_tokens = (resid.astype(F32) + (combined + combined_other.astype(F32))).astype(BF16)
    return (next_tokens, new_memory, new_normalizer, new_stab)


def solution(mesh):
    fine = Mesh(mesh.devices.reshape(Z, Y, XH, C, TP), (*EP, "tp"))
    ep = EP
    return jax.shard_map(
        local,
        mesh=fine,
        in_specs=(
            P(ep, None),
            P(),
            P(None, "tp"),
            P(None, "tp"),
            P(None, "tp"),
            P(None, "tp"),
            P(),
            P(),
            P(),
            P(),
            P("tp", None),
            P(ep, "tp", None, None),
            P(ep, "tp", None),
            P(ep, "tp"),
            P(),
            P(ep, None),
            P(ep, None),
            P(ep, None, "tp"),
            P(ep, None, "tp"),
            P(ep, "tp", None),
        ),
        out_specs=(P(ep, None), P(ep, "tp", None, None), P(ep, "tp", None), P(ep, "tp")),
        check_vma=False,
    )
```

```python
import jax
import jax.numpy as jnp
from jax import lax
from jax.experimental import pallas as pl
from jax.experimental.pallas import tpu as pltpu
from jax.sharding import Mesh, PartitionSpec as P

EPS = 1e-06
Z, Y, XH, C, TP = 8, 4, 2, 2, 2
EP = ("z", "y", "xh", "c")
F32, BF16 = jnp.float32, jnp.bfloat16
PAD = 16


def plane_pairs(dy, dx, back):
    pairs = []
    for y in range(Y):
        for xh in range(XH):
            for t in range(TP):
                src = (y * XH + xh) * TP + t
                dst = (((y + dy) % Y) * XH + (xh ^ dx)) * TP + (t ^ dx)
                pairs.append((dst, src) if back else (src, dst))
    return pairs


STEPS = [(dy, dx) for dy in range(Y) for dx in range(XH)]


def plane_exchange(parts, back):
    out = []
    for (dy, dx), part in zip(STEPS, parts):
        if dy == 0 and dx == 0:
            out.append(part)
        else:
            out.append(lax.ppermute(part, ("y", "xh", "tp"), plane_pairs(dy, dx, back)))
    return out


SWAP = [(0, 1), (1, 0)]


def cell_kernel(*refs):
    ins, outs, scr = refs[:14], refs[14:18], refs[18:]
    vm = scr[:14]
    out_v = (outs[0], *scr[14:17])
    num_v, gate_v, in_sem, mem_sem, out_sem = scr[17:]
    mem, mem_v = ins[13], vm[13]
    new_mem_hbm, new_mem_v = outs[1], out_v[1]
    rows = 12
    first = (0, 1, 2, 3, 4, 5, 6, 7, 8, 9, 10, 11)
    copies = {i: pltpu.make_async_copy(ins[i], vm[i], in_sem.at[i]) for i in (*first, 12)}
    mem_copies = [pltpu.make_async_copy(mem.at[b], mem_v.at[b], mem_sem.at[b]) for b in range(rows)]
    for i in first:
        copies[i].start()
    for cp in mem_copies:
        cp.start()
    copies[12].start()
    (tok, gain, stab, nrm, bias, hgain, wig, wfg, wk, wq, wv, wo, wout, _) = vm
    copies[0].wait()
    copies[1].wait()
    x = tok[...].astype(F32)
    normed = (x * lax.rsqrt(jnp.mean(x * x, axis=-1, keepdims=True) + EPS) * gain[...]).astype(BF16)
    for i in range(2, 8):
        copies[i].wait()
    first_half = lax.axis_index("tp") == 0

    def own(weights):
        both = lax.dot_general(weights[...], normed, (((1,), (1,)), ((), ())), preferred_element_type=F32)
        return jnp.where(first_half, both[0:2], both[2:4])

    input_pre = own(wig)
    biases = bias[...]
    column = lax.broadcasted_iota(jnp.int32, (2, rows), 0)
    low_bias = jnp.where(first_half, biases[:, 0:1], biases[:, 2:3])
    high_bias = jnp.where(first_half, biases[:, 1:2], biases[:, 3:4])
    forget = own(wfg) + jnp.where(column == 0, low_bias, high_bias)
    log_forget = jnp.minimum(forget, 0.0) - jnp.log1p(jnp.exp(-jnp.abs(forget)))
    carried = log_forget + stab[...]
    new_stab = jnp.maximum(carried, input_pre)
    out_v[3][...] = new_stab
    gate_v[...] = jnp.zeros((8, 128), F32)
    gate_v[0:2, 0:rows] = jnp.exp(carried - new_stab)
    gate_v[2:4, 0:rows] = jnp.exp(input_pre - new_stab)
    gate_v[4:6, 0:rows] = jnp.exp(-new_stab)
    gates = jnp.transpose(gate_v[...])[0:rows]
    keep, write, floor = gates[:, 0:2], gates[:, 2:4], gates[:, 4:6]
    copies[8].wait()
    key = jnp.dot(normed, wk[...], preferred_element_type=F32) * 192 ** (-0.5)
    head = lax.broadcasted_iota(jnp.int32, (rows, 384), 1) >= 192
    wkey = jnp.where(head, write[:, 1:2], write[:, 0:1]) * key

    def turned(values):
        return jnp.transpose(jnp.concatenate([values, jnp.zeros((128 - rows, 384), F32)], axis=0))

    wkey_t = turned(wkey)
    copies[9].wait()
    query = jnp.dot(normed, wq[...], preferred_element_type=F32)
    query_t = turned(query)
    copies[10].wait()
    value = jnp.dot(normed, wv[...], preferred_element_type=F32)
    copies[11].wait()
    outgate = jnp.dot(normed, wo[...], preferred_element_type=F32)
    gain_rows = jnp.where(first_half, hgain[0:3, :], hgain[3:6, :])
    gains = jnp.concatenate([gain_rows[i : i + 1] for i in range(3)], axis=1)
    cut = lambda v, h: v[:, h * 192 : (h + 1) * 192]
    values = [cut(value, h) for h in range(2)]
    keeps = [jnp.broadcast_to(keep[:, h : h + 1], (rows, 192)) for h in range(2)]
    floors = []
    for h in range(2):
        new_norm = keeps[h] * nrm[:, h, :] + cut(wkey, h)
        out_v[2][:, h, :] = new_norm
        den = jnp.sum(cut(query, h) * new_norm, axis=-1, keepdims=True)
        floors.append(jnp.maximum(jnp.abs(den), floor[:, h : h + 1]))
    out_copies = []
    for b in range(rows):
        mem_copies[b].wait()
        for h in range(2):
            span = slice(h * 192, (h + 1) * 192)
            updated = keeps[h][b : b + 1] * mem_v[b, h] + wkey_t[span, b : b + 1] * values[h][b : b + 1]
            new_mem_v[b, h] = updated
            num_v[h, b : b + 1, :] = jnp.sum(query_t[span, b : b + 1] * updated, axis=0, keepdims=True)
        cp = pltpu.make_async_copy(new_mem_v.at[b], new_mem_hbm.at[b], mem_sem.at[b])
        cp.start()
        out_copies.append(cp)
    total = None
    copies[12].wait()
    for h in range(2):
        readout = num_v[h] / floors[h]
        scaled = readout * lax.rsqrt(jnp.mean(readout * readout, axis=-1, keepdims=True) + EPS) * cut(gains, h)
        gated = (scaled * jax.nn.sigmoid(cut(outgate, h))).astype(BF16)
        part = jnp.dot(gated, wout[h * 192 : (h + 1) * 192, :], preferred_element_type=F32)
        total = part if total is None else total + part
    out_v[0][...] = total.astype(BF16)
    for i in (2, 3):
        cp = pltpu.make_async_copy(out_v[i], outs[i], out_sem.at[i])
        cp.start()
        out_copies.append(cp)
    for cp in out_copies:
        cp.wait()


def cell(tokens, gain, stab, nrm, bias, hgain, wig, wfg, wk, wq, wv, wo, wout, memory):
    args = (tokens, gain, stab, nrm, bias, hgain, wig, wfg, wk, wq, wv, wo, wout, memory)
    outs = [
        pltpu.VMEM((12, 2048), BF16),
        jax.ShapeDtypeStruct(memory.shape, F32),
        jax.ShapeDtypeStruct(nrm.shape, F32),
        jax.ShapeDtypeStruct(stab.shape, F32),
    ]
    scratch = [pltpu.VMEM(a.shape, a.dtype) for a in args] + [pltpu.VMEM(o.shape, o.dtype) for o in outs[1:]]
    scratch += [
        pltpu.VMEM((2, 12, 192), F32),
        pltpu.VMEM((8, 128), F32),
        pltpu.SemaphoreType.DMA((14,)),
        pltpu.SemaphoreType.DMA((12,)),
        pltpu.SemaphoreType.DMA((4,)),
    ]
    return pl.pallas_call(
        cell_kernel,
        out_shape=outs,
        in_specs=[pl.BlockSpec(memory_space=pl.ANY)] * len(args),
        out_specs=[pl.BlockSpec(memory_space=pltpu.VMEM)] + [pl.BlockSpec(memory_space=pl.ANY)] * 3,
        scratch_shapes=scratch,
        name="cell",
    )(*args)


def near(x):
    return pltpu.with_memory_space_constraint(x, pltpu.VMEM)


WHOLE = pl.BlockSpec(memory_space=pltpu.VMEM)
HALF, META = 1024, 1152
SIDE = Z * 24


def mix_kernel(tok, mine, other, gain, ids, probs, block_out, resid_out, scr):
    mixed = (mine[...].astype(F32) + other[...].astype(F32)).astype(BF16)
    resid = (tok[...].astype(F32) + mixed.astype(F32)).astype(BF16)
    resid_out[...] = resid
    x = resid.astype(F32)
    normed = x * lax.rsqrt(jnp.mean(x * x, axis=-1, keepdims=True) + EPS) * gain[...]
    weights = probs[...] / jnp.sum(probs[...], axis=0, keepdims=True)
    high = weights.astype(BF16)
    low = (weights - high.astype(F32)).astype(BF16)
    lane = lax.broadcasted_iota(jnp.int32, (4, 128), 1)
    row = lax.broadcasted_iota(jnp.int32, (4, 128), 0)
    meta = jnp.zeros((12, 128), F32)
    for i, v in enumerate(((ids[...] + 1).astype(F32).astype(BF16), high, low)):
        place = (lane == row + 4 * i).astype(F32).astype(BF16)
        meta = meta + lax.dot_general(v, place, (((0,), (0,)), ((), ())), preferred_element_type=F32)
    for h in range(2):
        scr[h * 12 : h * 12 + 12, 0:HALF] = normed[:, h * HALF : (h + 1) * HALF]
        scr[h * 12 : h * 12 + 12, HALF:META] = meta
    block = scr[...].astype(BF16)
    for j in range(Z):
        block_out[j] = block


def mix(tokens, mine, other, gain, ids, probs):
    return pl.pallas_call(
        mix_kernel,
        out_shape=[pltpu.VMEM((Z, 24, META), BF16), pltpu.VMEM((12, 2048), BF16)],
        in_specs=[WHOLE] * 6,
        out_specs=[WHOLE] * 2,
        scratch_shapes=[pltpu.VMEM((24, META), F32)],
        name="mix",
    )(near(tokens), near(mine), near(other), near(gain), near(ids), near(probs))


def pack_kernel(col_a, col_b, *refs):
    sent, weights_out = refs[:8], refs[8]
    z, y, xh, c = (lax.axis_index(a) for a in EP)
    row = lax.broadcasted_iota(jnp.int32, (128, SIDE), 0)
    lane = lax.broadcasted_iota(jnp.int32, (128, SIDE), 1)
    dy, dx = row >> 5, (row >> 4) & 1
    expert = ((z * Y + ((y + dy) & 3)) * XH + (xh ^ dx)) * C + c + 1
    expert = expert.astype(F32)
    pick = (
        lax.broadcasted_iota(jnp.int32, (16, 128), 1) == lax.broadcasted_iota(jnp.int32, (16, 128), 0)
    ).astype(F32).astype(BF16)
    group = (lane * 171) >> 11
    origin = lax.broadcasted_iota(jnp.int32, (SIDE, SIDE), 0)
    target = lax.broadcasted_iota(jnp.int32, (SIDE, SIDE), 1)
    before = (((origin * 171) >> 11) == ((target * 171) >> 11)) & (origin < target)
    before = before.astype(F32).astype(BF16)
    same = ((row >> 1) & 7) == (group >> 1)
    slot = (row & 1).astype(F32)
    halves = [(group & 1) == h for h in range(2)]
    for side, col in enumerate((col_a, col_b)):
        found = lax.dot_general(
            pick, col[:, HALF:META], (((1,), (1,)), ((), ())), preferred_element_type=F32
        )
        hit = jnp.zeros((128, SIDE), F32)
        w_high = jnp.zeros((128, SIDE), F32)
        w_low = jnp.zeros((128, SIDE), F32)
        for k in range(4):
            match = found[k : k + 1] == expert
            hit = hit + jnp.where(match, 1.0, 0.0)
            w_high = w_high + jnp.where(match, found[4 + k : 5 + k], 0.0)
            w_low = w_low + jnp.where(match, found[8 + k : 9 + k], 0.0)
        earlier = jnp.dot(hit.astype(BF16), before, preferred_element_type=F32)
        mask = same & (earlier == slot)
        for h in range(2):
            part = mask & halves[h]
            weights_out[side, h, 0] = jnp.where(part, w_high, 0.0).astype(BF16)
            weights_out[side, h, 1] = jnp.where(part, w_low, 0.0).astype(BF16)
            chosen = jnp.dot(
                jnp.where(part, hit, 0.0).astype(BF16), col[:, 0:HALF], preferred_element_type=F32
            ).astype(BF16)
            for j in range(8):
                sent[j][side * 16 : (side + 1) * 16, h * HALF : (h + 1) * HALF] = chosen[
                    j * 16 : (j + 1) * 16
                ]


def pack(col_a, col_b):
    return pl.pallas_call(
        pack_kernel,
        out_shape=[pltpu.VMEM((32, 2048), BF16)] * 8 + [pltpu.VMEM((2, 2, 2, 128, SIDE), BF16)],
        in_specs=[WHOLE] * 2,
        out_specs=[WHOLE] * 9,
        name="pack",
    )(near(col_a), near(col_b))


def combine_kernel(weights, *refs):
    back, (sum_a, sum_b), scr = refs[:8], refs[8:10], refs[10]
    dims = (((0,), (0,)), ((), ()))
    for side, out in ((1, sum_b), (0, sum_a)):
        for j in range(8):
            scr[side, j * 16 : (j + 1) * 16, :] = back[j][side * 16 : (side + 1) * 16, :]
        total = jnp.zeros((SIDE, HALF), F32)
        for h in range(2):
            values = scr[side, :, h * HALF : (h + 1) * HALF]
            for i in range(2):
                total = total + lax.dot_general(weights[side, h, i], values, dims, preferred_element_type=F32)
        out[...] = total.astype(out.dtype)


def combine(weights, back):
    return pl.pallas_call(
        combine_kernel,
        out_shape=[pltpu.VMEM((SIDE, HALF), F32), pltpu.VMEM((SIDE, HALF), BF16)],
        in_specs=[WHOLE] * 9,
        out_specs=[WHOLE] * 2,
        scratch_shapes=[pltpu.VMEM((2, 128, 2048), BF16)],
        name="combine",
    )(near(weights), *(near(b) for b in back))


def add_kernel(mine, other, out):
    out[...] = (mine[...] + other[...].astype(F32)).astype(BF16)


def add(mine, other):
    return pl.pallas_call(
        add_kernel,
        out_shape=pltpu.VMEM(mine.shape, BF16),
        in_specs=[WHOLE] * 2,
        out_specs=WHOLE,
        name="add",
    )(near(mine), near(other))


def gather_kernel(parts, total_out, sent_out):
    total = parts[0].astype(F32)
    for j in range(1, Z):
        total = total + parts[j].astype(F32)
    total_out[...] = total
    sent_out[...] = total.astype(BF16)


def gather(parts):
    return pl.pallas_call(
        gather_kernel,
        out_shape=[pltpu.VMEM((24, HALF), F32), pltpu.VMEM((24, HALF), BF16)],
        in_specs=[WHOLE],
        out_specs=[WHOLE] * 2,
        name="gather",
    )(near(parts))


def finish_kernel(resid, mine, other, out, scr):
    scr[...] = mine[...] + other[...].astype(F32)
    for h in range(2):
        cols = slice(h * HALF, (h + 1) * HALF)
        out[:, cols] = (resid[:, cols].astype(F32) + scr[h * 12 : h * 12 + 12, :]).astype(BF16)


def finish(resid, mine, other):
    return pl.pallas_call(
        finish_kernel,
        out_shape=jax.ShapeDtypeStruct((12, 2048), BF16),
        in_specs=[WHOLE] * 3,
        scratch_shapes=[pltpu.VMEM((24, HALF), F32)],
        name="finish",
    )(near(resid), near(mine), near(other))


def expert_kernel(*refs):
    rows, weights, outs = refs[:8], refs[8:11], refs[11:19]
    x, gate, up, down, sem = refs[19:]
    pieces = 2
    size = 512 // pieces
    copies = []
    for i in range(pieces):
        span = pl.ds(i * size, size)
        for k, dst in enumerate((gate, up, down)):
            if k < 2:
                cp = pltpu.make_async_copy(weights[k].at[0, :, span], dst.at[:, span], sem.at[k, i])
            else:
                cp = pltpu.make_async_copy(weights[k].at[0, span, :], dst.at[span, :], sem.at[k, i])
            cp.start()
            copies.append(cp)
    for j in range(8):
        x[j * 32 : (j + 1) * 32, :] = rows[j][...]
    total = None
    for i in range(pieces):
        span = slice(i * size, (i + 1) * size)
        copies[3 * i].wait()
        gate_val = jnp.dot(x[...], gate[:, span], preferred_element_type=F32)
        copies[3 * i + 1].wait()
        up_val = jnp.dot(x[...], up[:, span], preferred_element_type=F32)
        hidden = (gate_val * jax.nn.sigmoid(gate_val) * up_val).astype(BF16)
        copies[3 * i + 2].wait()
        part = jnp.dot(hidden, down[span, :], preferred_element_type=F32)
        total = part if total is None else total + part
    for j in range(8):
        outs[j][...] = total[j * 32 : (j + 1) * 32, :].astype(BF16)


def expert(rows, gate, up, down):
    return pl.pallas_call(
        expert_kernel,
        out_shape=[pltpu.VMEM((32, 2048), BF16)] * 8,
        in_specs=[WHOLE] * 8 + [pl.BlockSpec(memory_space=pl.ANY)] * 3,
        out_specs=[WHOLE] * 8,
        scratch_shapes=[
            pltpu.VMEM((256, 2048), BF16),
            pltpu.VMEM((2048, 512), BF16),
            pltpu.VMEM((2048, 512), BF16),
            pltpu.VMEM((512, 2048), BF16),
            pltpu.SemaphoreType.DMA((3, 2)),
        ],
        name="expert",
    )(*(near(r) for r in rows), gate, up, down)


def local(
    tokens,
    norm_gain,
    w_query,
    w_key,
    w_value,
    w_outgate,
    w_input_gate,
    w_forget_gate,
    forget_bias,
    head_gain,
    w_output,
    memory,
    normalizer,
    stabilizer,
    ffn_gain,
    route_ids,
    route_probs,
    expert_gate,
    expert_up,
    expert_down,
):
    partial_value, new_memory, new_normalizer, new_stab = cell(
        tokens,
        norm_gain.reshape(1, -1),
        stabilizer.T,
        normalizer,
        forget_bias.reshape(1, -1),
        head_gain.reshape(6, 128),
        w_input_gate.T,
        w_forget_gate.T,
        w_key,
        w_query,
        w_value,
        w_outgate,
        w_output,
        memory,
    )
    other_value = lax.ppermute(partial_value, "tp", SWAP)
    blocks, resid = mix(tokens, partial_value, other_value, ffn_gain.reshape(1, -1), route_ids.T, route_probs.T)
    column = lax.all_to_all(blocks, "z", 0, 0, tiled=True).reshape(SIDE, META)
    column_other = lax.ppermute(column, "c", SWAP)
    *sent, weights = pack(column, column_other)
    incoming = plane_exchange(sent, False)
    outgoing = expert(incoming, expert_gate, expert_up, expert_down)
    back = plane_exchange(outgoing, True)
    sum_a, sum_b = combine(weights, back)
    sum_b = lax.ppermute(sum_b, "c", SWAP)
    sums = add(sum_a, sum_b).reshape(Z, 24, HALF)
    sums = lax.all_to_all(sums, "z", 0, 0, tiled=True)
    combined, sent_on = gather(sums)
    combined_other = lax.ppermute(sent_on, "tp", SWAP)
    next_tokens = finish(resid, combined, combined_other)
    return (next_tokens, new_memory, new_normalizer, new_stab.T)


def solution(mesh):
    fine = Mesh(mesh.devices.reshape(Z, Y, XH, C, TP), (*EP, "tp"))
    ep = EP
    return jax.shard_map(
        local,
        mesh=fine,
        in_specs=(
            P(ep, None),
            P(),
            P(None, "tp"),
            P(None, "tp"),
            P(None, "tp"),
            P(None, "tp"),
            P(),
            P(),
            P(),
            P(),
            P("tp", None),
            P(ep, "tp", None, None),
            P(ep, "tp", None),
            P(ep, "tp"),
            P(),
            P(ep, None),
            P(ep, None),
            P(ep, None, "tp"),
            P(ep, None, "tp"),
            P(ep, "tp", None),
        ),
        out_specs=(P(ep, None), P(ep, "tp", None, None), P(ep, "tp", None), P(ep, "tp")),
        check_vma=False,
    )
```

```python
import functools

import jax
import jax.numpy as jnp
from jax import lax
from jax.experimental import pallas as pl
from jax.experimental.pallas import tpu as pltpu
from jax.sharding import Mesh, PartitionSpec as P

EPS = 1e-06
Z, Y, XH, C, TP = 8, 4, 2, 2, 2
EP = ("z", "y", "xh", "c")
F32, BF16 = jnp.float32, jnp.bfloat16
MIB = 1 << 20


def plane_pairs(dy, dx, back):
    pairs = []
    for y in range(Y):
        for xh in range(XH):
            for t in range(TP):
                src = (y * XH + xh) * TP + t
                dst = (((y + dy) % Y) * XH + (xh ^ dx)) * TP + (t ^ dx)
                pairs.append((dst, src) if back else (src, dst))
    return pairs


STEPS = [(0, 0), (2, 0), (0, 1), (2, 1), (1, 0), (1, 1), (3, 0), (3, 1)]


def plane_exchange(parts, back):
    out = []
    for (dy, dx), part in zip(STEPS, parts):
        if dy == 0 and dx == 0:
            out.append(part)
        else:
            out.append(lax.ppermute(part, ("y", "xh", "tp"), plane_pairs(dy, dx, back)))
    return out


SWAP = [(0, 1), (1, 0)]


def cell_kernel(*refs):
    ins, outs, scr = refs[:14], refs[14:21], refs[21:]
    part_out, mem_v, wkey_out, value_out, keep_out, norm_hbm, stab_hbm = outs
    vm = scr[:13]
    norm_v, stab_v, num_v, gate_v, in_sem, mem_sem, out_sem = scr[13:]
    mem = ins[13]
    rows = 12
    copies = [pltpu.make_async_copy(ins[i], vm[i], in_sem.at[i]) for i in range(13)]
    mem_copies = [pltpu.make_async_copy(mem.at[b], mem_v.at[b], mem_sem.at[b]) for b in range(rows)]
    for i in range(9):
        copies[i].start()
    for cp in mem_copies:
        cp.start()
    for i in range(9, 13):
        copies[i].start()
    (tok, gain, stab, nrm, bias, hgain, wig, wfg, wq, wk, wv, wo, wout) = vm
    copies[0].wait()
    copies[1].wait()
    x = tok[...].astype(F32)
    normed = (x * lax.rsqrt(jnp.mean(x * x, axis=-1, keepdims=True) + EPS) * gain[...]).astype(BF16)
    for i in range(2, 8):
        copies[i].wait()
    first_half = lax.axis_index("tp") == 0

    def own(weights):
        both = lax.dot_general(weights[...], normed, (((1,), (1,)), ((), ())), preferred_element_type=F32)
        return jnp.where(first_half, both[0:2], both[2:4])

    input_pre = own(wig)
    biases = bias[...]
    column = lax.broadcasted_iota(jnp.int32, (2, rows), 0)
    low_bias = jnp.where(first_half, biases[:, 0:1], biases[:, 2:3])
    high_bias = jnp.where(first_half, biases[:, 1:2], biases[:, 3:4])
    forget = own(wfg) + jnp.where(column == 0, low_bias, high_bias)
    log_forget = jnp.minimum(forget, 0.0) - jnp.log1p(jnp.exp(-jnp.abs(forget)))
    carried = log_forget + stab[...]
    new_stab = jnp.maximum(carried, input_pre)
    stab_v[...] = new_stab
    stab_copy = pltpu.make_async_copy(stab_v, stab_hbm, out_sem.at[0])
    stab_copy.start()
    gate_v[...] = jnp.zeros((8, 128), F32)
    gate_v[0:2, 0:rows] = jnp.exp(carried - new_stab)
    gate_v[2:4, 0:rows] = jnp.exp(input_pre - new_stab)
    gate_v[4:6, 0:rows] = jnp.exp(-new_stab)
    gates = jnp.transpose(gate_v[...])[0:rows]
    keep, write, floor = gates[:, 0:2], gates[:, 2:4], gates[:, 4:6]
    cut = lambda v, h: v[:, h * 192 : (h + 1) * 192]
    keeps = [jnp.broadcast_to(keep[:, h : h + 1], (rows, 192)) for h in range(2)]

    def turned(values):
        return jnp.transpose(jnp.concatenate([values, jnp.zeros((128 - rows, 384), F32)], axis=0))

    copies[8].wait()
    query = jnp.dot(normed, wq[...], preferred_element_type=F32)
    query_t = turned(query)
    for b in range(rows):
        mem_copies[b].wait()
        for h in range(2):
            span = slice(h * 192, (h + 1) * 192)
            num_v[h, b : b + 1, :] = jnp.sum(query_t[span, b : b + 1] * mem_v[b, h], axis=0, keepdims=True)
    copies[9].wait()
    key = jnp.dot(normed, wk[...], preferred_element_type=F32) * 192 ** (-0.5)
    head = lax.broadcasted_iota(jnp.int32, (rows, 384), 1) >= 192
    wkey = jnp.where(head, write[:, 1:2], write[:, 0:1]) * key
    wkey_out[...] = turned(wkey)
    scales, mixes = [], []
    for h in range(2):
        keep_out[h] = keeps[h]
        new_norm = keeps[h] * nrm[:, h, :] + cut(wkey, h)
        norm_v[:, h, :] = new_norm
        den = jnp.sum(cut(query, h) * new_norm, axis=-1, keepdims=True)
        scales.append(jnp.maximum(jnp.abs(den), floor[:, h : h + 1]))
        mixes.append(jnp.sum(cut(query, h) * cut(wkey, h), axis=-1, keepdims=True))
    norm_copy = pltpu.make_async_copy(norm_v, norm_hbm, out_sem.at[1])
    norm_copy.start()
    copies[10].wait()
    value = jnp.dot(normed, wv[...], preferred_element_type=F32)
    copies[11].wait()
    outgate = jnp.dot(normed, wo[...], preferred_element_type=F32)
    gain_rows = jnp.where(first_half, hgain[0:3, :], hgain[3:6, :])
    gains = jnp.concatenate([gain_rows[i : i + 1] for i in range(3)], axis=1)
    total = None
    copies[12].wait()
    for h in range(2):
        own_value = cut(value, h)
        value_out[h] = own_value
        readout = (keeps[h] * num_v[h] + mixes[h] * own_value) / scales[h]
        scaled = readout * lax.rsqrt(jnp.mean(readout * readout, axis=-1, keepdims=True) + EPS) * cut(gains, h)
        gated = (scaled * jax.nn.sigmoid(cut(outgate, h))).astype(BF16)
        part = jnp.dot(gated, wout[h * 192 : (h + 1) * 192, :], preferred_element_type=F32)
        total = part if total is None else total + part
    part_out[...] = total.astype(BF16)
    stab_copy.wait()
    norm_copy.wait()


ANYWHERE = pl.BlockSpec(memory_space=pl.ANY)
WHOLE = pl.BlockSpec(memory_space=pltpu.VMEM)


def cell(*args):
    memory, nrm, stab = args[13], args[3], args[2]
    outs = [
        pltpu.VMEM((12, 2048), BF16),
        pltpu.VMEM(memory.shape, F32),
        pltpu.VMEM((384, 128), F32),
        pltpu.VMEM((2, 12, 192), F32),
        pltpu.VMEM((2, 12, 192), F32),
        jax.ShapeDtypeStruct(nrm.shape, F32),
        jax.ShapeDtypeStruct(stab.shape, F32),
    ]
    scratch = [pltpu.VMEM(a.shape, a.dtype) for a in args[:13]]
    scratch += [
        pltpu.VMEM(nrm.shape, F32),
        pltpu.VMEM(stab.shape, F32),
        pltpu.VMEM((2, 12, 192), F32),
        pltpu.VMEM((8, 128), F32),
        pltpu.SemaphoreType.DMA((13,)),
        pltpu.SemaphoreType.DMA((12,)),
        pltpu.SemaphoreType.DMA((2,)),
    ]
    return pl.pallas_call(
        cell_kernel,
        out_shape=outs,
        in_specs=[ANYWHERE] * 14,
        out_specs=[WHOLE] * 5 + [ANYWHERE] * 2,
        scratch_shapes=scratch,
        name="cell",
        compiler_params=pltpu.CompilerParams(vmem_limit_bytes=24 * MIB),
    )(*(pltpu.with_memory_space_constraint(a, pltpu.HBM) for a in args))


def update_kernel(mem, wkey_t, value, keep, order, out, done, new_v, sem):
    done[...] = jnp.zeros((8, 128), F32)
    copies = []
    for b in range(12):
        for h in range(2):
            span = slice(h * 192, (h + 1) * 192)
            new_v[b, h] = (
                keep[h, b : b + 1, :] * mem[b, h] + wkey_t[span, b : b + 1] * value[h, b : b + 1, :]
            )
        cp = pltpu.make_async_copy(new_v.at[b], out.at[b], sem.at[b])
        cp.start()
        copies.append(cp)
    for cp in copies:
        cp.wait()


def update(mem, wkey_t, value, keep, order):
    return pl.pallas_call(
        update_kernel,
        out_shape=[jax.ShapeDtypeStruct(mem.shape, F32), pltpu.VMEM((8, 128), F32)],
        in_specs=[WHOLE] * 5,
        out_specs=[ANYWHERE, WHOLE],
        scratch_shapes=[pltpu.VMEM(mem.shape, F32), pltpu.SemaphoreType.DMA((12,))],
        name="update",
        compiler_params=pltpu.CompilerParams(vmem_limit_bytes=12 * MIB),
    )(near(mem), near(wkey_t), near(value), near(keep), near(order))


def load_kernel(gate, up, down, order, gate_v, up_v, down_v, sem):
    copies = [
        pltpu.make_async_copy(src.at[0], dst, sem.at[i])
        for i, (src, dst) in enumerate(((gate, gate_v), (up, up_v), (down, down_v)))
    ]
    for cp in copies:
        cp.start()
    for cp in copies:
        cp.wait()


def load(gate, up, down, order):
    return pl.pallas_call(
        load_kernel,
        out_shape=[pltpu.VMEM(w.shape[1:], BF16) for w in (gate, up, down)],
        in_specs=[ANYWHERE] * 3 + [WHOLE],
        out_specs=[WHOLE] * 3,
        scratch_shapes=[pltpu.SemaphoreType.DMA((3,))],
        name="load",
        compiler_params=pltpu.CompilerParams(vmem_limit_bytes=4 * MIB),
    )(*(pltpu.with_memory_space_constraint(w, pltpu.HBM) for w in (gate, up, down)), near(order))


def near(x):
    return pltpu.with_memory_space_constraint(x, pltpu.VMEM)


HALF, META = 1024, 1152
SIDE = Z * 24


def mix_kernel(tok, mine, other, gain, ids, probs, block_out, resid_out, scr):
    mixed = (mine[...].astype(F32) + other[...].astype(F32)).astype(BF16)
    resid = (tok[...].astype(F32) + mixed.astype(F32)).astype(BF16)
    resid_out[...] = resid
    x = resid.astype(F32)
    normed = x * lax.rsqrt(jnp.mean(x * x, axis=-1, keepdims=True) + EPS) * gain[...]
    weights = probs[...] / jnp.sum(probs[...], axis=0, keepdims=True)
    high = weights.astype(BF16)
    low = (weights - high.astype(F32)).astype(BF16)
    lane = lax.broadcasted_iota(jnp.int32, (4, 128), 1)
    row = lax.broadcasted_iota(jnp.int32, (4, 128), 0)
    meta = jnp.zeros((12, 128), F32)
    for i, v in enumerate(((ids[...] + 1).astype(F32).astype(BF16), high, low)):
        place = (lane == row + 4 * i).astype(F32).astype(BF16)
        meta = meta + lax.dot_general(v, place, (((0,), (0,)), ((), ())), preferred_element_type=F32)
    for h in range(2):
        scr[h * 12 : h * 12 + 12, 0:HALF] = normed[:, h * HALF : (h + 1) * HALF]
        scr[h * 12 : h * 12 + 12, HALF:META] = meta
    block = scr[...].astype(BF16)
    for j in range(Z):
        block_out[j] = block


def mix(tokens, mine, other, gain, ids, probs):
    return pl.pallas_call(
        mix_kernel,
        out_shape=[pltpu.VMEM((Z, 24, META), BF16), pltpu.VMEM((12, 2048), BF16)],
        in_specs=[WHOLE] * 6,
        out_specs=[WHOLE] * 2,
        scratch_shapes=[pltpu.VMEM((24, META), F32)],
        name="mix",
        compiler_params=pltpu.CompilerParams(vmem_limit_bytes=8 * MIB),
    )(near(tokens), near(mine), near(other), near(gain), near(ids), near(probs))


def pack_kernel(col_a, col_b, *refs):
    sent, weights_out = refs[:8], refs[8]
    z, y, xh, c = (lax.axis_index(a) for a in EP)
    row = lax.broadcasted_iota(jnp.int32, (128, SIDE), 0)
    lane = lax.broadcasted_iota(jnp.int32, (128, SIDE), 1)
    dy, dx = jnp.zeros_like(row), jnp.zeros_like(row)
    for j, (step_y, step_x) in enumerate(STEPS):
        dy = jnp.where((row >> 4) == j, step_y, dy)
        dx = jnp.where((row >> 4) == j, step_x, dx)
    expert = ((z * Y + ((y + dy) & 3)) * XH + (xh ^ dx)) * C + c + 1
    expert = expert.astype(F32)
    pick = (
        lax.broadcasted_iota(jnp.int32, (16, 128), 1) == lax.broadcasted_iota(jnp.int32, (16, 128), 0)
    ).astype(F32).astype(BF16)
    group = (lane * 171) >> 11
    origin = lax.broadcasted_iota(jnp.int32, (SIDE, SIDE), 0)
    target = lax.broadcasted_iota(jnp.int32, (SIDE, SIDE), 1)
    before = (((origin * 171) >> 11) == ((target * 171) >> 11)) & (origin < target)
    before = before.astype(F32).astype(BF16)
    same = ((row >> 1) & 7) == (group >> 1)
    slot = (row & 1).astype(F32)
    halves = [(group & 1) == h for h in range(2)]
    for side, col in enumerate((col_a, col_b)):
        found = lax.dot_general(
            pick, col[:, HALF:META], (((1,), (1,)), ((), ())), preferred_element_type=F32
        )
        hit = jnp.zeros((128, SIDE), F32)
        w_high = jnp.zeros((128, SIDE), F32)
        w_low = jnp.zeros((128, SIDE), F32)
        for k in range(4):
            match = found[k : k + 1] == expert
            hit = hit + jnp.where(match, 1.0, 0.0)
            w_high = w_high + jnp.where(match, found[4 + k : 5 + k], 0.0)
            w_low = w_low + jnp.where(match, found[8 + k : 9 + k], 0.0)
        earlier = jnp.dot(hit.astype(BF16), before, preferred_element_type=F32)
        mask = same & (earlier == slot)
        for h in range(2):
            part = mask & halves[h]
            weights_out[side, h, 0] = jnp.where(part, w_high, 0.0).astype(BF16)
            weights_out[side, h, 1] = jnp.where(part, w_low, 0.0).astype(BF16)
            chosen = jnp.dot(
                jnp.where(part, hit, 0.0).astype(BF16), col[:, 0:HALF], preferred_element_type=F32
            ).astype(BF16)
            for j in range(8):
                sent[j][side * 16 : (side + 1) * 16, h * HALF : (h + 1) * HALF] = chosen[
                    j * 16 : (j + 1) * 16
                ]


def pack(col_a, col_b):
    return pl.pallas_call(
        pack_kernel,
        out_shape=[pltpu.VMEM((32, 2048), BF16)] * 8 + [pltpu.VMEM((2, 2, 2, 128, SIDE), BF16)],
        in_specs=[WHOLE] * 2,
        out_specs=[WHOLE] * 9,
        name="pack",
        compiler_params=pltpu.CompilerParams(vmem_limit_bytes=12 * MIB),
    )(near(col_a), near(col_b))


def combine_kernel(side, weights, order, *refs):
    back, out, scr = refs[:8], refs[8], refs[9]
    dims = (((0,), (0,)), ((), ()))
    for j in range(8):
        scr[j * 16 : (j + 1) * 16, :] = back[j][side * 16 : (side + 1) * 16, :]
    total = jnp.zeros((SIDE, HALF), F32)
    for h in range(2):
        values = scr[:, h * HALF : (h + 1) * HALF]
        for i in range(2):
            total = total + lax.dot_general(weights[side, h, i], values, dims, preferred_element_type=F32)
    out[...] = total.astype(out.dtype)


def combine(weights, order, back, side, dtype):
    return pl.pallas_call(
        functools.partial(combine_kernel, side),
        out_shape=pltpu.VMEM((SIDE, HALF), dtype),
        in_specs=[WHOLE] * 10,
        out_specs=WHOLE,
        scratch_shapes=[pltpu.VMEM((128, 2048), BF16)],
        name="combine",
        compiler_params=pltpu.CompilerParams(vmem_limit_bytes=12 * MIB),
    )(near(weights), near(order), *(near(b) for b in back))


def add_kernel(mine, other, out):
    out[...] = (mine[...] + other[...].astype(F32)).astype(BF16)


def add(mine, other):
    return pl.pallas_call(
        add_kernel,
        out_shape=pltpu.VMEM(mine.shape, BF16),
        in_specs=[WHOLE] * 2,
        out_specs=WHOLE,
        name="add",
        compiler_params=pltpu.CompilerParams(vmem_limit_bytes=8 * MIB),
    )(near(mine), near(other))


def gather_kernel(parts, total_out, sent_out):
    total = parts[0].astype(F32)
    for j in range(1, Z):
        total = total + parts[j].astype(F32)
    total_out[...] = total
    sent_out[...] = total.astype(BF16)


def gather(parts):
    return pl.pallas_call(
        gather_kernel,
        out_shape=[pltpu.VMEM((24, HALF), F32), pltpu.VMEM((24, HALF), BF16)],
        in_specs=[WHOLE],
        out_specs=[WHOLE] * 2,
        name="gather",
        compiler_params=pltpu.CompilerParams(vmem_limit_bytes=8 * MIB),
    )(near(parts))


def finish_kernel(resid, mine, other, out, scr):
    scr[...] = mine[...] + other[...].astype(F32)
    for h in range(2):
        cols = slice(h * HALF, (h + 1) * HALF)
        out[:, cols] = (resid[:, cols].astype(F32) + scr[h * 12 : h * 12 + 12, :]).astype(BF16)


def finish(resid, mine, other):
    return pl.pallas_call(
        finish_kernel,
        out_shape=jax.ShapeDtypeStruct((12, 2048), BF16),
        in_specs=[WHOLE] * 3,
        scratch_shapes=[pltpu.VMEM((24, HALF), F32)],
        name="finish",
        compiler_params=pltpu.CompilerParams(vmem_limit_bytes=8 * MIB),
    )(near(resid), near(mine), near(other))


def expert_kernel(*refs):
    rows, (gate, up, down), outs, x = refs[:8], refs[8:11], refs[11:19], refs[19]
    for j in range(8):
        x[j * 32 : (j + 1) * 32, :] = rows[j][...]
    gate_val = jnp.dot(x[...], gate[...], preferred_element_type=F32)
    up_val = jnp.dot(x[...], up[...], preferred_element_type=F32)
    hidden = (gate_val * jax.nn.sigmoid(gate_val) * up_val).astype(BF16)
    total = jnp.dot(hidden, down[...], preferred_element_type=F32)
    for j in range(8):
        outs[j][...] = total[j * 32 : (j + 1) * 32, :].astype(BF16)


def expert(rows, weights):
    return pl.pallas_call(
        expert_kernel,
        out_shape=[pltpu.VMEM((32, 2048), BF16)] * 8,
        in_specs=[WHOLE] * 11,
        out_specs=[WHOLE] * 8,
        scratch_shapes=[pltpu.VMEM((256, 2048), BF16)],
        name="expert",
        compiler_params=pltpu.CompilerParams(vmem_limit_bytes=20 * MIB),
    )(*(near(r) for r in rows), *(near(w) for w in weights))


def local(
    tokens,
    norm_gain,
    w_query,
    w_key,
    w_value,
    w_outgate,
    w_input_gate,
    w_forget_gate,
    forget_bias,
    head_gain,
    w_output,
    memory,
    normalizer,
    stabilizer,
    ffn_gain,
    route_ids,
    route_probs,
    expert_gate,
    expert_up,
    expert_down,
):
    partial_value, mem_near, wkey_t, value, keep, new_normalizer, new_stab = cell(
        tokens,
        norm_gain.reshape(1, -1),
        stabilizer.T,
        normalizer,
        forget_bias.reshape(1, -1),
        head_gain.reshape(6, 128),
        w_input_gate.T,
        w_forget_gate.T,
        w_query,
        w_key,
        w_value,
        w_outgate,
        w_output,
        memory,
    )
    other_value = lax.ppermute(partial_value, "tp", SWAP)
    blocks, resid = mix(tokens, partial_value, other_value, ffn_gain.reshape(1, -1), route_ids.T, route_probs.T)
    column = lax.all_to_all(blocks, "z", 0, 0, tiled=True).reshape(SIDE, META)
    column_other = lax.ppermute(column, "c", SWAP)
    *sent, weights = pack(column, column_other)
    incoming = plane_exchange(sent, False)
    outgoing = expert(incoming, load(expert_gate, expert_up, expert_down, weights))
    back = plane_exchange(outgoing, True)
    new_memory, order = update(mem_near, wkey_t, value, keep, outgoing[0])
    sum_b = lax.ppermute(combine(weights, order, back, 1, BF16), "c", SWAP)
    sum_a = combine(weights, order, back, 0, F32)
    sums = add(sum_a, sum_b).reshape(Z, 24, HALF)
    sums = lax.all_to_all(sums, "z", 0, 0, tiled=True)
    combined, sent_on = gather(sums)
    combined_other = lax.ppermute(sent_on, "tp", SWAP)
    next_tokens = finish(resid, combined, combined_other)
    return (next_tokens, new_memory, new_normalizer, new_stab.T)


def solution(mesh):
    fine = Mesh(mesh.devices.reshape(Z, Y, XH, C, TP), (*EP, "tp"))
    ep = EP
    return jax.shard_map(
        local,
        mesh=fine,
        in_specs=(
            P(ep, None),
            P(),
            P(None, "tp"),
            P(None, "tp"),
            P(None, "tp"),
            P(None, "tp"),
            P(),
            P(),
            P(),
            P(),
            P("tp", None),
            P(ep, "tp", None, None),
            P(ep, "tp", None),
            P(ep, "tp"),
            P(),
            P(ep, None),
            P(ep, None),
            P(ep, None, "tp"),
            P(ep, None, "tp"),
            P(ep, "tp", None),
        ),
        out_specs=(P(ep, None), P(ep, "tp", None, None), P(ep, "tp", None), P(ep, "tp")),
        check_vma=False,
    )
```

```python
import functools

import jax
import jax.numpy as jnp
from jax import lax
from jax.experimental import pallas as pl
from jax.experimental.pallas import tpu as pltpu
from jax.sharding import Mesh, PartitionSpec as P

EPS = 1e-06
Z, Y, XH, C, TP = 8, 4, 2, 2, 2
EP = ("z", "y", "xh", "c")
F32, BF16 = jnp.float32, jnp.bfloat16
MIB = 1 << 20


def plane_pairs(dy, dx, back):
    pairs = []
    for y in range(Y):
        for xh in range(XH):
            for t in range(TP):
                src = (y * XH + xh) * TP + t
                dst = (((y + dy) % Y) * XH + (xh ^ dx)) * TP + (t ^ dx)
                pairs.append((dst, src) if back else (src, dst))
    return pairs


STEPS = [(0, 0), (2, 0), (0, 1), (2, 1), (1, 0), (1, 1), (3, 0), (3, 1)]


def plane_exchange(parts, back):
    out = []
    for (dy, dx), part in zip(STEPS, parts):
        if dy == 0 and dx == 0:
            out.append(part)
        else:
            out.append(lax.ppermute(part, ("y", "xh", "tp"), plane_pairs(dy, dx, back)))
    return out


SWAP = [(0, 1), (1, 0)]


def cell_kernel(*refs):
    ins, outs, scr = refs[:14], refs[14:21], refs[21:]
    part_out, mem_v, wkey_out, value_out, keep_out, norm_hbm, stab_hbm = outs
    vm = scr[:13]
    norm_v, stab_v, num_v, gate_v, in_sem, mem_sem, out_sem = scr[13:]
    mem = ins[13]
    rows = 12
    copies = [pltpu.make_async_copy(ins[i], vm[i], in_sem.at[i]) for i in range(13)]
    mem_copies = [pltpu.make_async_copy(mem.at[b], mem_v.at[b], mem_sem.at[b]) for b in range(rows)]
    for i in range(12):
        copies[i].start()
    for cp in mem_copies:
        cp.start()
    copies[12].start()
    (tok, gain, stab, nrm, bias, hgain, wig, wfg, wq, wk, wv, wo, wout) = vm
    copies[0].wait()
    copies[1].wait()
    x = tok[...].astype(F32)
    normed = (x * lax.rsqrt(jnp.mean(x * x, axis=-1, keepdims=True) + EPS) * gain[...]).astype(BF16)
    for i in range(2, 8):
        copies[i].wait()
    first_half = lax.axis_index("tp") == 0

    def own(weights):
        both = lax.dot_general(weights[...], normed, (((1,), (1,)), ((), ())), preferred_element_type=F32)
        return jnp.where(first_half, both[0:2], both[2:4])

    input_pre = own(wig)
    biases = bias[...]
    column = lax.broadcasted_iota(jnp.int32, (2, rows), 0)
    low_bias = jnp.where(first_half, biases[:, 0:1], biases[:, 2:3])
    high_bias = jnp.where(first_half, biases[:, 1:2], biases[:, 3:4])
    forget = own(wfg) + jnp.where(column == 0, low_bias, high_bias)
    log_forget = jnp.minimum(forget, 0.0) - jnp.log1p(jnp.exp(-jnp.abs(forget)))
    carried = log_forget + stab[...]
    new_stab = jnp.maximum(carried, input_pre)
    stab_v[...] = new_stab
    stab_copy = pltpu.make_async_copy(stab_v, stab_hbm, out_sem.at[0])
    stab_copy.start()
    gate_v[...] = jnp.zeros((8, 128), F32)
    gate_v[0:2, 0:rows] = jnp.exp(carried - new_stab)
    gate_v[2:4, 0:rows] = jnp.exp(input_pre - new_stab)
    gate_v[4:6, 0:rows] = jnp.exp(-new_stab)
    gates = jnp.transpose(gate_v[...])[0:rows]
    keep, write, floor = gates[:, 0:2], gates[:, 2:4], gates[:, 4:6]
    cut = lambda v, h: v[:, h * 192 : (h + 1) * 192]
    keeps = [jnp.broadcast_to(keep[:, h : h + 1], (rows, 192)) for h in range(2)]

    def turned(values):
        return jnp.transpose(jnp.concatenate([values, jnp.zeros((128 - rows, 384), F32)], axis=0))

    copies[8].wait()
    query = jnp.dot(normed, wq[...], preferred_element_type=F32)
    query_t = turned(query)
    copies[9].wait()
    key = jnp.dot(normed, wk[...], preferred_element_type=F32) * 192 ** (-0.5)
    head = lax.broadcasted_iota(jnp.int32, (rows, 384), 1) >= 192
    wkey = jnp.where(head, write[:, 1:2], write[:, 0:1]) * key
    wkey_out[...] = turned(wkey)
    scales, mixes = [], []
    for h in range(2):
        keep_out[h] = keeps[h]
        new_norm = keeps[h] * nrm[:, h, :] + cut(wkey, h)
        norm_v[:, h, :] = new_norm
        den = jnp.sum(cut(query, h) * new_norm, axis=-1, keepdims=True)
        scales.append(jnp.maximum(jnp.abs(den), floor[:, h : h + 1]))
        mixes.append(jnp.sum(cut(query, h) * cut(wkey, h), axis=-1, keepdims=True))
    norm_copy = pltpu.make_async_copy(norm_v, norm_hbm, out_sem.at[1])
    norm_copy.start()
    copies[10].wait()
    value = jnp.dot(normed, wv[...], preferred_element_type=F32)
    copies[11].wait()
    outgate = jnp.dot(normed, wo[...], preferred_element_type=F32)
    gain_rows = jnp.where(first_half, hgain[0:3, :], hgain[3:6, :])
    gains = jnp.concatenate([gain_rows[i : i + 1] for i in range(3)], axis=1)
    own_values = [cut(value, h) for h in range(2)]
    shapes = [jax.nn.sigmoid(cut(outgate, h)) for h in range(2)]
    for h in range(2):
        value_out[h] = own_values[h]
    for b in range(rows):
        mem_copies[b].wait()
        for h in range(2):
            span = slice(h * 192, (h + 1) * 192)
            num_v[h, b : b + 1, :] = jnp.sum(query_t[span, b : b + 1] * mem_v[b, h], axis=0, keepdims=True)
    total = None
    copies[12].wait()
    for h in range(2):
        readout = (keeps[h] * num_v[h] + mixes[h] * own_values[h]) / scales[h]
        scaled = readout * lax.rsqrt(jnp.mean(readout * readout, axis=-1, keepdims=True) + EPS) * cut(gains, h)
        gated = (scaled * shapes[h]).astype(BF16)
        part = jnp.dot(gated, wout[h * 192 : (h + 1) * 192, :], preferred_element_type=F32)
        total = part if total is None else total + part
    part_out[...] = total.astype(BF16)
    stab_copy.wait()
    norm_copy.wait()


ANYWHERE = pl.BlockSpec(memory_space=pl.ANY)
WHOLE = pl.BlockSpec(memory_space=pltpu.VMEM)


def cell(*args):
    memory, nrm, stab = args[13], args[3], args[2]
    outs = [
        pltpu.VMEM((12, 2048), BF16),
        pltpu.VMEM(memory.shape, F32),
        pltpu.VMEM((384, 128), F32),
        pltpu.VMEM((2, 12, 192), F32),
        pltpu.VMEM((2, 12, 192), F32),
        jax.ShapeDtypeStruct(nrm.shape, F32),
        jax.ShapeDtypeStruct(stab.shape, F32),
    ]
    scratch = [pltpu.VMEM(a.shape, a.dtype) for a in args[:13]]
    scratch += [
        pltpu.VMEM(nrm.shape, F32),
        pltpu.VMEM(stab.shape, F32),
        pltpu.VMEM((2, 12, 192), F32),
        pltpu.VMEM((8, 128), F32),
        pltpu.SemaphoreType.DMA((13,)),
        pltpu.SemaphoreType.DMA((12,)),
        pltpu.SemaphoreType.DMA((2,)),
    ]
    return pl.pallas_call(
        cell_kernel,
        out_shape=outs,
        in_specs=[ANYWHERE] * 14,
        out_specs=[WHOLE] * 5 + [ANYWHERE] * 2,
        scratch_shapes=scratch,
        name="cell",
        compiler_params=pltpu.CompilerParams(vmem_limit_bytes=24 * MIB),
    )(*(pltpu.with_memory_space_constraint(a, pltpu.HBM) for a in args))


def update_kernel(mem, wkey_t, value, keep, order, out, done, new_v, sem):
    done[...] = jnp.zeros((8, 128), F32)
    copies = []
    for b in range(12):
        for h in range(2):
            span = slice(h * 192, (h + 1) * 192)
            new_v[b, h] = (
                keep[h, b : b + 1, :] * mem[b, h] + wkey_t[span, b : b + 1] * value[h, b : b + 1, :]
            )
        cp = pltpu.make_async_copy(new_v.at[b], out.at[b], sem.at[b])
        cp.start()
        copies.append(cp)
    for cp in copies:
        cp.wait()


def update(mem, wkey_t, value, keep, order):
    return pl.pallas_call(
        update_kernel,
        out_shape=[jax.ShapeDtypeStruct(mem.shape, F32), pltpu.VMEM((8, 128), F32)],
        in_specs=[WHOLE] * 5,
        out_specs=[ANYWHERE, WHOLE],
        scratch_shapes=[pltpu.VMEM(mem.shape, F32), pltpu.SemaphoreType.DMA((12,))],
        name="update",
        compiler_params=pltpu.CompilerParams(vmem_limit_bytes=12 * MIB),
    )(near(mem), near(wkey_t), near(value), near(keep), near(order))


def load_kernel(gate, up, down, order, gate_v, up_v, down_v, sem):
    copies = [
        pltpu.make_async_copy(src.at[0], dst, sem.at[i])
        for i, (src, dst) in enumerate(((gate, gate_v), (up, up_v), (down, down_v)))
    ]
    for cp in copies:
        cp.start()
    for cp in copies:
        cp.wait()


def load(gate, up, down, order):
    return pl.pallas_call(
        load_kernel,
        out_shape=[pltpu.VMEM(w.shape[1:], BF16) for w in (gate, up, down)],
        in_specs=[ANYWHERE] * 3 + [WHOLE],
        out_specs=[WHOLE] * 3,
        scratch_shapes=[pltpu.SemaphoreType.DMA((3,))],
        name="load",
        compiler_params=pltpu.CompilerParams(vmem_limit_bytes=4 * MIB),
    )(*(pltpu.with_memory_space_constraint(w, pltpu.HBM) for w in (gate, up, down)), near(order))


def near(x):
    return pltpu.with_memory_space_constraint(x, pltpu.VMEM)


HALF, META = 1024, 1152
SIDE = Z * 24


def mix_kernel(tok, mine, other, gain, ids, probs, block_out, resid_out, scr):
    mixed = (mine[...].astype(F32) + other[...].astype(F32)).astype(BF16)
    resid = (tok[...].astype(F32) + mixed.astype(F32)).astype(BF16)
    resid_out[...] = resid
    x = resid.astype(F32)
    normed = x * lax.rsqrt(jnp.mean(x * x, axis=-1, keepdims=True) + EPS) * gain[...]
    weights = probs[...] / jnp.sum(probs[...], axis=0, keepdims=True)
    high = weights.astype(BF16)
    low = (weights - high.astype(F32)).astype(BF16)
    lane = lax.broadcasted_iota(jnp.int32, (4, 128), 1)
    row = lax.broadcasted_iota(jnp.int32, (4, 128), 0)
    meta = jnp.zeros((12, 128), F32)
    for i, v in enumerate(((ids[...] + 1).astype(F32).astype(BF16), high, low)):
        place = (lane == row + 4 * i).astype(F32).astype(BF16)
        meta = meta + lax.dot_general(v, place, (((0,), (0,)), ((), ())), preferred_element_type=F32)
    for h in range(2):
        scr[h * 12 : h * 12 + 12, 0:HALF] = normed[:, h * HALF : (h + 1) * HALF]
        scr[h * 12 : h * 12 + 12, HALF:META] = meta
    block = scr[...].astype(BF16)
    for j in range(Z):
        block_out[j] = block


def mix(tokens, mine, other, gain, ids, probs):
    return pl.pallas_call(
        mix_kernel,
        out_shape=[pltpu.VMEM((Z, 24, META), BF16), pltpu.VMEM((12, 2048), BF16)],
        in_specs=[WHOLE] * 6,
        out_specs=[WHOLE] * 2,
        scratch_shapes=[pltpu.VMEM((24, META), F32)],
        name="mix",
        compiler_params=pltpu.CompilerParams(vmem_limit_bytes=8 * MIB),
    )(near(tokens), near(mine), near(other), near(gain), near(ids), near(probs))


def pack_kernel(col_a, col_b, *refs):
    sent, weights_out = refs[:8], refs[8]
    z, y, xh, c = (lax.axis_index(a) for a in EP)
    row = lax.broadcasted_iota(jnp.int32, (128, SIDE), 0)
    lane = lax.broadcasted_iota(jnp.int32, (128, SIDE), 1)
    dy, dx = jnp.zeros_like(row), jnp.zeros_like(row)
    for j, (step_y, step_x) in enumerate(STEPS):
        dy = jnp.where((row >> 4) == j, step_y, dy)
        dx = jnp.where((row >> 4) == j, step_x, dx)
    expert = ((z * Y + ((y + dy) & 3)) * XH + (xh ^ dx)) * C + c + 1
    expert = expert.astype(F32)
    pick = (
        lax.broadcasted_iota(jnp.int32, (16, 128), 1) == lax.broadcasted_iota(jnp.int32, (16, 128), 0)
    ).astype(F32).astype(BF16)
    group = (lane * 171) >> 11
    origin = lax.broadcasted_iota(jnp.int32, (SIDE, SIDE), 0)
    target = lax.broadcasted_iota(jnp.int32, (SIDE, SIDE), 1)
    before = (((origin * 171) >> 11) == ((target * 171) >> 11)) & (origin < target)
    before = before.astype(F32).astype(BF16)
    same = ((row >> 1) & 7) == (group >> 1)
    slot = (row & 1).astype(F32)
    halves = [(group & 1) == h for h in range(2)]
    for side, col in enumerate((col_a, col_b)):
        found = lax.dot_general(
            pick, col[:, HALF:META], (((1,), (1,)), ((), ())), preferred_element_type=F32
        )
        hit = jnp.zeros((128, SIDE), F32)
        w_high = jnp.zeros((128, SIDE), F32)
        w_low = jnp.zeros((128, SIDE), F32)
        for k in range(4):
            match = found[k : k + 1] == expert
            hit = hit + jnp.where(match, 1.0, 0.0)
            w_high = w_high + jnp.where(match, found[4 + k : 5 + k], 0.0)
            w_low = w_low + jnp.where(match, found[8 + k : 9 + k], 0.0)
        earlier = jnp.dot(hit.astype(BF16), before, preferred_element_type=F32)
        mask = same & (earlier == slot)
        for h in range(2):
            part = mask & halves[h]
            weights_out[side, h, 0] = jnp.where(part, w_high, 0.0).astype(BF16)
            weights_out[side, h, 1] = jnp.where(part, w_low, 0.0).astype(BF16)
            chosen = jnp.dot(
                jnp.where(part, hit, 0.0).astype(BF16), col[:, 0:HALF], preferred_element_type=F32
            ).astype(BF16)
            for j in range(8):
                sent[j][side * 16 : (side + 1) * 16, h * HALF : (h + 1) * HALF] = chosen[
                    j * 16 : (j + 1) * 16
                ]


def pack(col_a, col_b):
    return pl.pallas_call(
        pack_kernel,
        out_shape=[pltpu.VMEM((32, 2048), BF16)] * 8 + [pltpu.VMEM((2, 2, 2, 128, SIDE), BF16)],
        in_specs=[WHOLE] * 2,
        out_specs=[WHOLE] * 9,
        name="pack",
        compiler_params=pltpu.CompilerParams(vmem_limit_bytes=12 * MIB),
    )(near(col_a), near(col_b))


def combine_kernel(side, weights, order, *refs):
    back, out, scr = refs[:8], refs[8], refs[9]
    dims = (((0,), (0,)), ((), ()))
    for j in range(8):
        scr[j * 16 : (j + 1) * 16, :] = back[j][side * 16 : (side + 1) * 16, :]
    total = jnp.zeros((SIDE, HALF), F32)
    for h in range(2):
        values = scr[:, h * HALF : (h + 1) * HALF]
        for i in range(2):
            total = total + lax.dot_general(weights[side, h, i], values, dims, preferred_element_type=F32)
    out[...] = total.astype(out.dtype)


def combine(weights, order, back, side, dtype):
    return pl.pallas_call(
        functools.partial(combine_kernel, side),
        out_shape=pltpu.VMEM((SIDE, HALF), dtype),
        in_specs=[WHOLE] * 10,
        out_specs=WHOLE,
        scratch_shapes=[pltpu.VMEM((128, 2048), BF16)],
        name="combine",
        compiler_params=pltpu.CompilerParams(vmem_limit_bytes=12 * MIB),
    )(near(weights), near(order), *(near(b) for b in back))


def add_kernel(mine, other, out):
    out[...] = (mine[...] + other[...].astype(F32)).astype(BF16)


def add(mine, other):
    return pl.pallas_call(
        add_kernel,
        out_shape=pltpu.VMEM(mine.shape, BF16),
        in_specs=[WHOLE] * 2,
        out_specs=WHOLE,
        name="add",
        compiler_params=pltpu.CompilerParams(vmem_limit_bytes=8 * MIB),
    )(near(mine), near(other))


def gather_kernel(parts, total_out, sent_out):
    total = parts[0].astype(F32)
    for j in range(1, Z):
        total = total + parts[j].astype(F32)
    total_out[...] = total
    sent_out[...] = total.astype(BF16)


def gather(parts):
    return pl.pallas_call(
        gather_kernel,
        out_shape=[pltpu.VMEM((24, HALF), F32), pltpu.VMEM((24, HALF), BF16)],
        in_specs=[WHOLE],
        out_specs=[WHOLE] * 2,
        name="gather",
        compiler_params=pltpu.CompilerParams(vmem_limit_bytes=8 * MIB),
    )(near(parts))


def finish_kernel(resid, mine, other, out, scr):
    scr[...] = mine[...] + other[...].astype(F32)
    for h in range(2):
        cols = slice(h * HALF, (h + 1) * HALF)
        out[:, cols] = (resid[:, cols].astype(F32) + scr[h * 12 : h * 12 + 12, :]).astype(BF16)


def finish(resid, mine, other):
    return pl.pallas_call(
        finish_kernel,
        out_shape=jax.ShapeDtypeStruct((12, 2048), BF16),
        in_specs=[WHOLE] * 3,
        scratch_shapes=[pltpu.VMEM((24, HALF), F32)],
        name="finish",
        compiler_params=pltpu.CompilerParams(vmem_limit_bytes=8 * MIB),
    )(near(resid), near(mine), near(other))


def expert_kernel(*refs):
    rows, (gate, up, down), outs, x = refs[:4], refs[4:7], refs[7:11], refs[11]
    for j in range(4):
        x[j * 32 : (j + 1) * 32, :] = rows[j][...]
    gate_val = jnp.dot(x[...], gate[...], preferred_element_type=F32)
    up_val = jnp.dot(x[...], up[...], preferred_element_type=F32)
    hidden = (gate_val * jax.nn.sigmoid(gate_val) * up_val).astype(BF16)
    total = jnp.dot(hidden, down[...], preferred_element_type=F32)
    for j in range(4):
        outs[j][...] = total[j * 32 : (j + 1) * 32, :].astype(BF16)


def expert(rows, weights):
    return pl.pallas_call(
        expert_kernel,
        out_shape=[pltpu.VMEM((32, 2048), BF16)] * 4,
        in_specs=[WHOLE] * 7,
        out_specs=[WHOLE] * 4,
        scratch_shapes=[pltpu.VMEM((128, 2048), BF16)],
        name="expert",
        compiler_params=pltpu.CompilerParams(vmem_limit_bytes=16 * MIB),
    )(*(near(r) for r in rows), *(near(w) for w in weights))


def local(
    tokens,
    norm_gain,
    w_query,
    w_key,
    w_value,
    w_outgate,
    w_input_gate,
    w_forget_gate,
    forget_bias,
    head_gain,
    w_output,
    memory,
    normalizer,
    stabilizer,
    ffn_gain,
    route_ids,
    route_probs,
    expert_gate,
    expert_up,
    expert_down,
):
    partial_value, mem_near, wkey_t, value, keep, new_normalizer, new_stab = cell(
        tokens,
        norm_gain.reshape(1, -1),
        stabilizer.T,
        normalizer,
        forget_bias.reshape(1, -1),
        head_gain.reshape(6, 128),
        w_input_gate.T,
        w_forget_gate.T,
        w_query,
        w_key,
        w_value,
        w_outgate,
        w_output,
        memory,
    )
    other_value = lax.ppermute(partial_value, "tp", SWAP)
    blocks, resid = mix(tokens, partial_value, other_value, ffn_gain.reshape(1, -1), route_ids.T, route_probs.T)
    column = lax.all_to_all(blocks, "z", 0, 0, tiled=True).reshape(SIDE, META)
    column_other = lax.ppermute(column, "c", SWAP)
    *sent, weights = pack(column, column_other)
    incoming = plane_exchange(sent, False)
    loaded = load(expert_gate, expert_up, expert_down, weights)
    outgoing = [*expert(incoming[:4], loaded), *expert(incoming[4:], loaded)]
    back = plane_exchange(outgoing, True)
    new_memory, order = update(mem_near, wkey_t, value, keep, outgoing[4])
    sum_b = lax.ppermute(combine(weights, order, back, 1, BF16), "c", SWAP)
    sum_a = combine(weights, order, back, 0, F32)
    sums = add(sum_a, sum_b).reshape(Z, 24, HALF)
    sums = lax.all_to_all(sums, "z", 0, 0, tiled=True)
    combined, sent_on = gather(sums)
    combined_other = lax.ppermute(sent_on, "tp", SWAP)
    next_tokens = finish(resid, combined, combined_other)
    return (next_tokens, new_memory, new_normalizer, new_stab.T)


def solution(mesh):
    fine = Mesh(mesh.devices.reshape(Z, Y, XH, C, TP), (*EP, "tp"))
    ep = EP
    return jax.shard_map(
        local,
        mesh=fine,
        in_specs=(
            P(ep, None),
            P(),
            P(None, "tp"),
            P(None, "tp"),
            P(None, "tp"),
            P(None, "tp"),
            P(),
            P(),
            P(),
            P(),
            P("tp", None),
            P(ep, "tp", None, None),
            P(ep, "tp", None),
            P(ep, "tp"),
            P(),
            P(ep, None),
            P(ep, None),
            P(ep, None, "tp"),
            P(ep, None, "tp"),
            P(ep, "tp", None),
        ),
        out_specs=(P(ep, None), P(ep, "tp", None, None), P(ep, "tp", None), P(ep, "tp")),
        check_vma=False,
    )
```

```python
import functools

import jax
import jax.numpy as jnp
from jax import lax
from jax.experimental import pallas as pl
from jax.experimental.pallas import tpu as pltpu
from jax.sharding import Mesh, PartitionSpec as P

EPS = 1e-06
Z, Y, XH, C, TP = 8, 4, 2, 2, 2
EP = ("z", "y", "xh", "c")
F32, BF16 = jnp.float32, jnp.bfloat16
MIB = 1 << 20


def plane_pairs(dy, dx, back):
    pairs = []
    for y in range(Y):
        for xh in range(XH):
            for t in range(TP):
                src = (y * XH + xh) * TP + t
                dst = (((y + dy) % Y) * XH + (xh ^ dx)) * TP + (t ^ dx)
                pairs.append((dst, src) if back else (src, dst))
    return pairs


STEPS = [(0, 0), (2, 0), (0, 1), (2, 1), (1, 0), (1, 1), (3, 0), (3, 1)]


def plane_exchange(parts, back):
    out = []
    for (dy, dx), part in zip(STEPS, parts):
        if dy == 0 and dx == 0:
            out.append(part)
        else:
            out.append(lax.ppermute(part, ("y", "xh", "tp"), plane_pairs(dy, dx, back)))
    return out


SWAP = [(0, 1), (1, 0)]


def cell_kernel(*refs):
    ins, outs, scr = refs[:14], refs[14:21], refs[21:]
    part_out, mem_v, wkey_out, value_out, keep_out, norm_hbm, stab_hbm = outs
    vm = scr[:13]
    norm_v, stab_v, num_v, gate_v, in_sem, mem_sem, out_sem = scr[13:]
    mem = ins[13]
    rows = 12
    copies = [pltpu.make_async_copy(ins[i], vm[i], in_sem.at[i]) for i in range(13)]
    mem_copies = [pltpu.make_async_copy(mem.at[b], mem_v.at[b], mem_sem.at[b]) for b in range(rows)]
    for i in range(12):
        copies[i].start()
    for cp in mem_copies:
        cp.start()
    copies[12].start()
    (tok, gain, stab, nrm, bias, hgain, wig, wfg, wq, wk, wv, wo, wout) = vm
    copies[0].wait()
    copies[1].wait()
    x = tok[...].astype(F32)
    normed = (x * lax.rsqrt(jnp.mean(x * x, axis=-1, keepdims=True) + EPS) * gain[...]).astype(BF16)
    for i in range(2, 8):
        copies[i].wait()
    first_half = lax.axis_index("tp") == 0

    def own(weights):
        both = lax.dot_general(weights[...], normed, (((1,), (1,)), ((), ())), preferred_element_type=F32)
        return jnp.where(first_half, both[0:2], both[2:4])

    input_pre = own(wig)
    biases = bias[...]
    column = lax.broadcasted_iota(jnp.int32, (2, rows), 0)
    low_bias = jnp.where(first_half, biases[:, 0:1], biases[:, 2:3])
    high_bias = jnp.where(first_half, biases[:, 1:2], biases[:, 3:4])
    forget = own(wfg) + jnp.where(column == 0, low_bias, high_bias)
    log_forget = jnp.minimum(forget, 0.0) - jnp.log1p(jnp.exp(-jnp.abs(forget)))
    carried = log_forget + stab[...]
    new_stab = jnp.maximum(carried, input_pre)
    stab_v[...] = new_stab
    stab_copy = pltpu.make_async_copy(stab_v, stab_hbm, out_sem.at[0])
    stab_copy.start()
    gate_v[...] = jnp.zeros((8, 128), F32)
    gate_v[0:2, 0:rows] = jnp.exp(carried - new_stab)
    gate_v[2:4, 0:rows] = jnp.exp(input_pre - new_stab)
    gate_v[4:6, 0:rows] = jnp.exp(-new_stab)
    gates = jnp.transpose(gate_v[...])[0:rows]
    keep, write, floor = gates[:, 0:2], gates[:, 2:4], gates[:, 4:6]
    cut = lambda v, h: v[:, h * 192 : (h + 1) * 192]
    keeps = [jnp.broadcast_to(keep[:, h : h + 1], (rows, 192)) for h in range(2)]

    def turned(values):
        return jnp.transpose(jnp.concatenate([values, jnp.zeros((128 - rows, 384), F32)], axis=0))

    copies[8].wait()
    query = jnp.dot(normed, wq[...], preferred_element_type=F32)
    query_t = turned(query)
    copies[9].wait()
    key = jnp.dot(normed, wk[...], preferred_element_type=F32) * 192 ** (-0.5)
    head = lax.broadcasted_iota(jnp.int32, (rows, 384), 1) >= 192
    wkey = jnp.where(head, write[:, 1:2], write[:, 0:1]) * key
    wkey_out[...] = turned(wkey)
    scales, mixes = [], []
    for h in range(2):
        keep_out[h] = keeps[h]
        new_norm = keeps[h] * nrm[:, h, :] + cut(wkey, h)
        norm_v[:, h, :] = new_norm
        den = jnp.sum(cut(query, h) * new_norm, axis=-1, keepdims=True)
        scales.append(jnp.maximum(jnp.abs(den), floor[:, h : h + 1]))
        mixes.append(jnp.sum(cut(query, h) * cut(wkey, h), axis=-1, keepdims=True))
    norm_copy = pltpu.make_async_copy(norm_v, norm_hbm, out_sem.at[1])
    norm_copy.start()
    copies[10].wait()
    value = jnp.dot(normed, wv[...], preferred_element_type=F32)
    copies[11].wait()
    outgate = jnp.dot(normed, wo[...], preferred_element_type=F32)
    gain_rows = jnp.where(first_half, hgain[0:3, :], hgain[3:6, :])
    gains = jnp.concatenate([gain_rows[i : i + 1] for i in range(3)], axis=1)
    own_values = [cut(value, h) for h in range(2)]
    shapes = [jax.nn.sigmoid(cut(outgate, h)) for h in range(2)]
    for h in range(2):
        value_out[h] = own_values[h]
    for b in range(rows):
        mem_copies[b].wait()
        for h in range(2):
            span = slice(h * 192, (h + 1) * 192)
            num_v[h, b : b + 1, :] = jnp.sum(query_t[span, b : b + 1] * mem_v[b, h], axis=0, keepdims=True)
    total = None
    copies[12].wait()
    for h in range(2):
        readout = (keeps[h] * num_v[h] + mixes[h] * own_values[h]) / scales[h]
        scaled = readout * lax.rsqrt(jnp.mean(readout * readout, axis=-1, keepdims=True) + EPS) * cut(gains, h)
        gated = (scaled * shapes[h]).astype(BF16)
        part = jnp.dot(gated, wout[h * 192 : (h + 1) * 192, :], preferred_element_type=F32)
        total = part if total is None else total + part
    part_out[...] = total.astype(BF16)
    stab_copy.wait()
    norm_copy.wait()


ANYWHERE = pl.BlockSpec(memory_space=pl.ANY)
WHOLE = pl.BlockSpec(memory_space=pltpu.VMEM)


def cell(*args):
    memory, nrm, stab = args[13], args[3], args[2]
    outs = [
        pltpu.VMEM((12, 2048), BF16),
        pltpu.VMEM(memory.shape, F32),
        pltpu.VMEM((384, 128), F32),
        pltpu.VMEM((2, 12, 192), F32),
        pltpu.VMEM((2, 12, 192), F32),
        jax.ShapeDtypeStruct(nrm.shape, F32),
        jax.ShapeDtypeStruct(stab.shape, F32),
    ]
    scratch = [pltpu.VMEM(a.shape, a.dtype) for a in args[:13]]
    scratch += [
        pltpu.VMEM(nrm.shape, F32),
        pltpu.VMEM(stab.shape, F32),
        pltpu.VMEM((2, 12, 192), F32),
        pltpu.VMEM((8, 128), F32),
        pltpu.SemaphoreType.DMA((13,)),
        pltpu.SemaphoreType.DMA((12,)),
        pltpu.SemaphoreType.DMA((2,)),
    ]
    return pl.pallas_call(
        cell_kernel,
        out_shape=outs,
        in_specs=[ANYWHERE] * 14,
        out_specs=[WHOLE] * 5 + [ANYWHERE] * 2,
        scratch_shapes=scratch,
        name="cell",
        compiler_params=pltpu.CompilerParams(vmem_limit_bytes=24 * MIB),
    )(*(pltpu.with_memory_space_constraint(a, pltpu.HBM) for a in args))


def update_kernel(mem, wkey_t, value, keep, order, out, done, new_v, sem):
    done[...] = jnp.zeros((8, 128), F32)
    copies = []
    for b in range(12):
        for h in range(2):
            span = slice(h * 192, (h + 1) * 192)
            new_v[b, h] = (
                keep[h, b : b + 1, :] * mem[b, h] + wkey_t[span, b : b + 1] * value[h, b : b + 1, :]
            )
        cp = pltpu.make_async_copy(new_v.at[b], out.at[b], sem.at[b])
        cp.start()
        copies.append(cp)
    for cp in copies:
        cp.wait()


def update(mem, wkey_t, value, keep, order):
    return pl.pallas_call(
        update_kernel,
        out_shape=[jax.ShapeDtypeStruct(mem.shape, F32), pltpu.VMEM((8, 128), F32)],
        in_specs=[WHOLE] * 5,
        out_specs=[ANYWHERE, WHOLE],
        scratch_shapes=[pltpu.VMEM(mem.shape, F32), pltpu.SemaphoreType.DMA((12,))],
        name="update",
        compiler_params=pltpu.CompilerParams(vmem_limit_bytes=12 * MIB),
    )(near(mem), near(wkey_t), near(value), near(keep), near(order))


def load_kernel(gate, up, down, order, gate_v, up_v, down_v, done, sem):
    done[...] = jnp.zeros((8, 128), F32)
    copies = [
        pltpu.make_async_copy(src.at[0], dst, sem.at[i])
        for i, (src, dst) in enumerate(((gate, gate_v), (up, up_v), (down, down_v)))
    ]
    for cp in copies:
        cp.start()
    for cp in copies:
        cp.wait()


def load(gate, up, down, order):
    return pl.pallas_call(
        load_kernel,
        out_shape=[*(pltpu.VMEM(w.shape[1:], BF16) for w in (gate, up, down)), pltpu.VMEM((8, 128), F32)],
        in_specs=[ANYWHERE] * 3 + [WHOLE],
        out_specs=[WHOLE] * 4,
        scratch_shapes=[pltpu.SemaphoreType.DMA((3,))],
        name="load",
        compiler_params=pltpu.CompilerParams(vmem_limit_bytes=4 * MIB),
    )(*(pltpu.with_memory_space_constraint(w, pltpu.HBM) for w in (gate, up, down)), near(order))


def near(x):
    return pltpu.with_memory_space_constraint(x, pltpu.VMEM)


HALF, META = 1024, 1152
SIDE = Z * 24


def mix_kernel(tok, mine, other, gain, ids, probs, order, block_out, resid_out, scr):
    mixed = (mine[...].astype(F32) + other[...].astype(F32)).astype(BF16)
    resid = (tok[...].astype(F32) + mixed.astype(F32)).astype(BF16)
    resid_out[...] = resid
    x = resid.astype(F32)
    normed = x * lax.rsqrt(jnp.mean(x * x, axis=-1, keepdims=True) + EPS) * gain[...]
    weights = probs[...] / jnp.sum(probs[...], axis=0, keepdims=True)
    high = weights.astype(BF16)
    low = (weights - high.astype(F32)).astype(BF16)
    lane = lax.broadcasted_iota(jnp.int32, (4, 128), 1)
    row = lax.broadcasted_iota(jnp.int32, (4, 128), 0)
    meta = jnp.zeros((12, 128), F32)
    for i, v in enumerate(((ids[...] + 1).astype(F32).astype(BF16), high, low)):
        place = (lane == row + 4 * i).astype(F32).astype(BF16)
        meta = meta + lax.dot_general(v, place, (((0,), (0,)), ((), ())), preferred_element_type=F32)
    for h in range(2):
        scr[h * 12 : h * 12 + 12, 0:HALF] = normed[:, h * HALF : (h + 1) * HALF]
        scr[h * 12 : h * 12 + 12, HALF:META] = meta
    block = scr[...].astype(BF16)
    for j in range(Z):
        block_out[j] = block


def mix(tokens, mine, other, gain, ids, probs, order):
    return pl.pallas_call(
        mix_kernel,
        out_shape=[pltpu.VMEM((Z, 24, META), BF16), pltpu.VMEM((12, 2048), BF16)],
        in_specs=[WHOLE] * 7,
        out_specs=[WHOLE] * 2,
        scratch_shapes=[pltpu.VMEM((24, META), F32)],
        name="mix",
        compiler_params=pltpu.CompilerParams(vmem_limit_bytes=8 * MIB),
    )(near(tokens), near(mine), near(other), near(gain), near(ids), near(probs), near(order))


def choose(col, weights_out):
    z, y, xh, c = (lax.axis_index(a) for a in EP)
    row = lax.broadcasted_iota(jnp.int32, (128, SIDE), 0)
    lane = lax.broadcasted_iota(jnp.int32, (128, SIDE), 1)
    dy, dx = jnp.zeros_like(row), jnp.zeros_like(row)
    for j, (step_y, step_x) in enumerate(STEPS):
        dy = jnp.where((row >> 4) == j, step_y, dy)
        dx = jnp.where((row >> 4) == j, step_x, dx)
    expert = ((z * Y + ((y + dy) & 3)) * XH + (xh ^ dx)) * C + c + 1
    expert = expert.astype(F32)
    pick = (
        lax.broadcasted_iota(jnp.int32, (16, 128), 1) == lax.broadcasted_iota(jnp.int32, (16, 128), 0)
    ).astype(F32).astype(BF16)
    group = (lane * 171) >> 11
    origin = lax.broadcasted_iota(jnp.int32, (SIDE, SIDE), 0)
    target = lax.broadcasted_iota(jnp.int32, (SIDE, SIDE), 1)
    before = (((origin * 171) >> 11) == ((target * 171) >> 11)) & (origin < target)
    before = before.astype(F32).astype(BF16)
    same = ((row >> 1) & 7) == (group >> 1)
    slot = (row & 1).astype(F32)
    found = lax.dot_general(pick, col[:, HALF:META], (((1,), (1,)), ((), ())), preferred_element_type=F32)
    hit = jnp.zeros((128, SIDE), F32)
    w_high = jnp.zeros((128, SIDE), F32)
    w_low = jnp.zeros((128, SIDE), F32)
    for k in range(4):
        match = found[k : k + 1] == expert
        hit = hit + jnp.where(match, 1.0, 0.0)
        w_high = w_high + jnp.where(match, found[4 + k : 5 + k], 0.0)
        w_low = w_low + jnp.where(match, found[8 + k : 9 + k], 0.0)
    earlier = jnp.dot(hit.astype(BF16), before, preferred_element_type=F32)
    mask = same & (earlier == slot)
    chosen = []
    for h in range(2):
        part = mask & ((group & 1) == h)
        weights_out[h, 0] = jnp.where(part, w_high, 0.0).astype(BF16)
        weights_out[h, 1] = jnp.where(part, w_low, 0.0).astype(BF16)
        chosen.append(
            jnp.dot(
                jnp.where(part, hit, 0.0).astype(BF16), col[:, 0:HALF], preferred_element_type=F32
            ).astype(BF16)
        )
    return chosen


WEIGHTS = (2, 2, 128, SIDE)


def pack_own_kernel(col, chosen_out, weights_out):
    for h, chosen in enumerate(choose(col, weights_out)):
        chosen_out[:, h * HALF : (h + 1) * HALF] = chosen


def pack_own(col):
    return pl.pallas_call(
        pack_own_kernel,
        out_shape=[pltpu.VMEM((128, 2048), BF16), pltpu.VMEM(WEIGHTS, BF16)],
        in_specs=[WHOLE],
        out_specs=[WHOLE] * 2,
        name="pack_own",
        compiler_params=pltpu.CompilerParams(vmem_limit_bytes=12 * MIB),
    )(near(col))


def pack_kernel(col, own, *refs):
    sent, weights_out = refs[:8], refs[8]
    for j in range(8):
        sent[j][0:16, :] = own[j * 16 : (j + 1) * 16, :]
    for h, chosen in enumerate(choose(col, weights_out)):
        for j in range(8):
            sent[j][16:32, h * HALF : (h + 1) * HALF] = chosen[j * 16 : (j + 1) * 16]


def pack(col, own):
    return pl.pallas_call(
        pack_kernel,
        out_shape=[pltpu.VMEM((32, 2048), BF16)] * 8 + [pltpu.VMEM(WEIGHTS, BF16)],
        in_specs=[WHOLE] * 2,
        out_specs=[WHOLE] * 9,
        name="pack",
        compiler_params=pltpu.CompilerParams(vmem_limit_bytes=12 * MIB),
    )(near(col), near(own))


def combine_kernel(side, weights, order, *refs):
    back, out, scr = refs[:8], refs[8], refs[9]
    dims = (((0,), (0,)), ((), ()))
    for j in range(8):
        scr[j * 16 : (j + 1) * 16, :] = back[j][side * 16 : (side + 1) * 16, :]
    total = jnp.zeros((SIDE, HALF), F32)
    for h in range(2):
        values = scr[:, h * HALF : (h + 1) * HALF]
        for i in range(2):
            total = total + lax.dot_general(weights[h, i], values, dims, preferred_element_type=F32)
    out[...] = total.astype(out.dtype)


def combine(weights, order, back, side, dtype):
    return pl.pallas_call(
        functools.partial(combine_kernel, side),
        out_shape=pltpu.VMEM((SIDE, HALF), dtype),
        in_specs=[WHOLE] * 10,
        out_specs=WHOLE,
        scratch_shapes=[pltpu.VMEM((128, 2048), BF16)],
        name="combine",
        compiler_params=pltpu.CompilerParams(vmem_limit_bytes=12 * MIB),
    )(near(weights), near(order), *(near(b) for b in back))


def add_kernel(mine, other, out):
    out[...] = (mine[...] + other[...].astype(F32)).astype(BF16)


def add(mine, other):
    return pl.pallas_call(
        add_kernel,
        out_shape=pltpu.VMEM(mine.shape, BF16),
        in_specs=[WHOLE] * 2,
        out_specs=WHOLE,
        name="add",
        compiler_params=pltpu.CompilerParams(vmem_limit_bytes=8 * MIB),
    )(near(mine), near(other))


def gather_kernel(parts, total_out, sent_out):
    total = parts[0].astype(F32)
    for j in range(1, Z):
        total = total + parts[j].astype(F32)
    total_out[...] = total
    sent_out[...] = total.astype(BF16)


def gather(parts):
    return pl.pallas_call(
        gather_kernel,
        out_shape=[pltpu.VMEM((24, HALF), F32), pltpu.VMEM((24, HALF), BF16)],
        in_specs=[WHOLE],
        out_specs=[WHOLE] * 2,
        name="gather",
        compiler_params=pltpu.CompilerParams(vmem_limit_bytes=8 * MIB),
    )(near(parts))


def finish_kernel(resid, mine, other, out, scr):
    scr[...] = mine[...] + other[...].astype(F32)
    for h in range(2):
        cols = slice(h * HALF, (h + 1) * HALF)
        out[:, cols] = (resid[:, cols].astype(F32) + scr[h * 12 : h * 12 + 12, :]).astype(BF16)


def finish(resid, mine, other):
    return pl.pallas_call(
        finish_kernel,
        out_shape=jax.ShapeDtypeStruct((12, 2048), BF16),
        in_specs=[WHOLE] * 3,
        scratch_shapes=[pltpu.VMEM((24, HALF), F32)],
        name="finish",
        compiler_params=pltpu.CompilerParams(vmem_limit_bytes=8 * MIB),
    )(near(resid), near(mine), near(other))


def expert_kernel(*refs):
    rows, (gate, up, down), outs, x = refs[:4], refs[4:7], refs[7:11], refs[11]
    for j in range(4):
        x[j * 32 : (j + 1) * 32, :] = rows[j][...]
    gate_val = jnp.dot(x[...], gate[...], preferred_element_type=F32)
    up_val = jnp.dot(x[...], up[...], preferred_element_type=F32)
    hidden = (gate_val * jax.nn.sigmoid(gate_val) * up_val).astype(BF16)
    total = jnp.dot(hidden, down[...], preferred_element_type=F32)
    for j in range(4):
        outs[j][...] = total[j * 32 : (j + 1) * 32, :].astype(BF16)


def expert(rows, weights):
    return pl.pallas_call(
        expert_kernel,
        out_shape=[pltpu.VMEM((32, 2048), BF16)] * 4,
        in_specs=[WHOLE] * 7,
        out_specs=[WHOLE] * 4,
        scratch_shapes=[pltpu.VMEM((128, 2048), BF16)],
        name="expert",
        compiler_params=pltpu.CompilerParams(vmem_limit_bytes=16 * MIB),
    )(*(near(r) for r in rows), *(near(w) for w in weights))


def local(
    tokens,
    norm_gain,
    w_query,
    w_key,
    w_value,
    w_outgate,
    w_input_gate,
    w_forget_gate,
    forget_bias,
    head_gain,
    w_output,
    memory,
    normalizer,
    stabilizer,
    ffn_gain,
    route_ids,
    route_probs,
    expert_gate,
    expert_up,
    expert_down,
):
    partial_value, mem_near, wkey_t, value, keep, new_normalizer, new_stab = cell(
        tokens,
        norm_gain.reshape(1, -1),
        stabilizer.T,
        normalizer,
        forget_bias.reshape(1, -1),
        head_gain.reshape(6, 128),
        w_input_gate.T,
        w_forget_gate.T,
        w_query,
        w_key,
        w_value,
        w_outgate,
        w_output,
        memory,
    )
    other_value = lax.ppermute(partial_value, "tp", SWAP)
    *loaded, order = load(expert_gate, expert_up, expert_down, partial_value)
    blocks, resid = mix(
        tokens, partial_value, other_value, ffn_gain.reshape(1, -1), route_ids.T, route_probs.T, order
    )
    column = lax.all_to_all(blocks, "z", 0, 0, tiled=True).reshape(SIDE, META)
    column_other = lax.ppermute(column, "c", SWAP)
    own, weights_own = pack_own(column)
    *sent, weights_other = pack(column_other, own)
    incoming = plane_exchange(sent, False)
    outgoing = [*expert(incoming[:4], loaded), *expert(incoming[4:], loaded)]
    back = plane_exchange(outgoing, True)
    new_memory, order = update(mem_near, wkey_t, value, keep, outgoing[4])
    sum_b = lax.ppermute(combine(weights_other, order, back, 1, BF16), "c", SWAP)
    sum_a = combine(weights_own, order, back, 0, F32)
    sums = add(sum_a, sum_b).reshape(Z, 24, HALF)
    sums = lax.all_to_all(sums, "z", 0, 0, tiled=True)
    combined, sent_on = gather(sums)
    combined_other = lax.ppermute(sent_on, "tp", SWAP)
    next_tokens = finish(resid, combined, combined_other)
    return (next_tokens, new_memory, new_normalizer, new_stab.T)


def solution(mesh):
    fine = Mesh(mesh.devices.reshape(Z, Y, XH, C, TP), (*EP, "tp"))
    ep = EP
    return jax.shard_map(
        local,
        mesh=fine,
        in_specs=(
            P(ep, None),
            P(),
            P(None, "tp"),
            P(None, "tp"),
            P(None, "tp"),
            P(None, "tp"),
            P(),
            P(),
            P(),
            P(),
            P("tp", None),
            P(ep, "tp", None, None),
            P(ep, "tp", None),
            P(ep, "tp"),
            P(),
            P(ep, None),
            P(ep, None),
            P(ep, None, "tp"),
            P(ep, None, "tp"),
            P(ep, "tp", None),
        ),
        out_specs=(P(ep, None), P(ep, "tp", None, None), P(ep, "tp", None), P(ep, "tp")),
        check_vma=False,
    )
```

```python
import functools

import jax
import jax.numpy as jnp
from jax import lax
from jax.experimental import pallas as pl
from jax.experimental.pallas import tpu as pltpu
from jax.sharding import Mesh, PartitionSpec as P

EPS = 1e-06
Z, Y, XH, C, TP = 8, 4, 2, 2, 2
EP = ("z", "y", "xh", "c")
F32, BF16 = jnp.float32, jnp.bfloat16
MIB = 1 << 20


def plane_pairs(dy, dx, back):
    pairs = []
    for y in range(Y):
        for xh in range(XH):
            for t in range(TP):
                src = (y * XH + xh) * TP + t
                dst = (((y + dy) % Y) * XH + (xh ^ dx)) * TP + (t ^ dx)
                pairs.append((dst, src) if back else (src, dst))
    return pairs


STEPS = [(0, 0), (2, 1), (2, 0), (0, 1), (1, 1), (3, 1), (1, 0), (3, 0)]


def plane_exchange(parts, back):
    out = []
    for (dy, dx), part in zip(STEPS, parts):
        if dy == 0 and dx == 0:
            out.append(part)
        else:
            out.append(lax.ppermute(part, ("y", "xh", "tp"), plane_pairs(dy, dx, back)))
    return out


SWAP = [(0, 1), (1, 0)]


def cell_kernel(*refs):
    ins, outs, scr = refs[:14], refs[14:21], refs[21:]
    part_out, mem_v, wkey_out, value_out, keep_out, norm_hbm, stab_hbm = outs
    vm = scr[:13]
    norm_v, stab_v, num_v, gate_v, in_sem, mem_sem, out_sem = scr[13:]
    mem = ins[13]
    rows = 12
    copies = [pltpu.make_async_copy(ins[i], vm[i], in_sem.at[i]) for i in range(13)]
    mem_copies = [pltpu.make_async_copy(mem.at[b], mem_v.at[b], mem_sem.at[b]) for b in range(rows)]
    for i in range(12):
        copies[i].start()
    for cp in mem_copies:
        cp.start()
    copies[12].start()
    (tok, gain, stab, nrm, bias, hgain, wig, wfg, wq, wk, wv, wo, wout) = vm
    copies[0].wait()
    copies[1].wait()
    x = tok[...].astype(F32)
    normed = (x * lax.rsqrt(jnp.mean(x * x, axis=-1, keepdims=True) + EPS) * gain[...]).astype(BF16)
    for i in range(2, 8):
        copies[i].wait()
    first_half = lax.axis_index("tp") == 0

    def own(weights):
        both = lax.dot_general(weights[...], normed, (((1,), (1,)), ((), ())), preferred_element_type=F32)
        return jnp.where(first_half, both[0:2], both[2:4])

    input_pre = own(wig)
    biases = bias[...]
    column = lax.broadcasted_iota(jnp.int32, (2, rows), 0)
    low_bias = jnp.where(first_half, biases[:, 0:1], biases[:, 2:3])
    high_bias = jnp.where(first_half, biases[:, 1:2], biases[:, 3:4])
    forget = own(wfg) + jnp.where(column == 0, low_bias, high_bias)
    log_forget = jnp.minimum(forget, 0.0) - jnp.log1p(jnp.exp(-jnp.abs(forget)))
    carried = log_forget + stab[...]
    new_stab = jnp.maximum(carried, input_pre)
    stab_v[...] = new_stab
    stab_copy = pltpu.make_async_copy(stab_v, stab_hbm, out_sem.at[0])
    stab_copy.start()
    gate_v[...] = jnp.zeros((8, 128), F32)
    gate_v[0:2, 0:rows] = jnp.exp(carried - new_stab)
    gate_v[2:4, 0:rows] = jnp.exp(input_pre - new_stab)
    gate_v[4:6, 0:rows] = jnp.exp(-new_stab)
    gates = jnp.transpose(gate_v[...])[0:rows]
    keep, write, floor = gates[:, 0:2], gates[:, 2:4], gates[:, 4:6]
    cut = lambda v, h: v[:, h * 192 : (h + 1) * 192]
    keeps = [jnp.broadcast_to(keep[:, h : h + 1], (rows, 192)) for h in range(2)]

    def turned(values):
        return jnp.transpose(jnp.concatenate([values, jnp.zeros((128 - rows, 384), F32)], axis=0))

    copies[8].wait()
    query = jnp.dot(normed, wq[...], preferred_element_type=F32)
    query_t = turned(query)
    copies[9].wait()
    key = jnp.dot(normed, wk[...], preferred_element_type=F32) * 192 ** (-0.5)
    head = lax.broadcasted_iota(jnp.int32, (rows, 384), 1) >= 192
    wkey = jnp.where(head, write[:, 1:2], write[:, 0:1]) * key
    wkey_out[...] = turned(wkey)
    scales, mixes = [], []
    for h in range(2):
        keep_out[h] = keeps[h]
        new_norm = keeps[h] * nrm[:, h, :] + cut(wkey, h)
        norm_v[:, h, :] = new_norm
        den = jnp.sum(cut(query, h) * new_norm, axis=-1, keepdims=True)
        scales.append(jnp.maximum(jnp.abs(den), floor[:, h : h + 1]))
        mixes.append(jnp.sum(cut(query, h) * cut(wkey, h), axis=-1, keepdims=True))
    norm_copy = pltpu.make_async_copy(norm_v, norm_hbm, out_sem.at[1])
    norm_copy.start()
    copies[10].wait()
    value = jnp.dot(normed, wv[...], preferred_element_type=F32)
    copies[11].wait()
    outgate = jnp.dot(normed, wo[...], preferred_element_type=F32)
    gain_rows = jnp.where(first_half, hgain[0:3, :], hgain[3:6, :])
    gains = jnp.concatenate([gain_rows[i : i + 1] for i in range(3)], axis=1)
    own_values = [cut(value, h) for h in range(2)]
    shapes = [jax.nn.sigmoid(cut(outgate, h)) for h in range(2)]
    for h in range(2):
        value_out[h] = own_values[h]
    for b in range(rows):
        mem_copies[b].wait()
        for h in range(2):
            span = slice(h * 192, (h + 1) * 192)
            num_v[h, b : b + 1, :] = jnp.sum(query_t[span, b : b + 1] * mem_v[b, h], axis=0, keepdims=True)
    total = None
    copies[12].wait()
    for h in range(2):
        readout = (keeps[h] * num_v[h] + mixes[h] * own_values[h]) / scales[h]
        scaled = readout * lax.rsqrt(jnp.mean(readout * readout, axis=-1, keepdims=True) + EPS) * cut(gains, h)
        gated = (scaled * shapes[h]).astype(BF16)
        part = jnp.dot(gated, wout[h * 192 : (h + 1) * 192, :], preferred_element_type=F32)
        total = part if total is None else total + part
    part_out[...] = total.astype(BF16)
    stab_copy.wait()
    norm_copy.wait()


ANYWHERE = pl.BlockSpec(memory_space=pl.ANY)
WHOLE = pl.BlockSpec(memory_space=pltpu.VMEM)


def cell(*args):
    memory, nrm, stab = args[13], args[3], args[2]
    outs = [
        pltpu.VMEM((12, 2048), BF16),
        pltpu.VMEM(memory.shape, F32),
        pltpu.VMEM((384, 128), F32),
        pltpu.VMEM((2, 12, 192), F32),
        pltpu.VMEM((2, 12, 192), F32),
        jax.ShapeDtypeStruct(nrm.shape, F32),
        jax.ShapeDtypeStruct(stab.shape, F32),
    ]
    scratch = [pltpu.VMEM(a.shape, a.dtype) for a in args[:13]]
    scratch += [
        pltpu.VMEM(nrm.shape, F32),
        pltpu.VMEM(stab.shape, F32),
        pltpu.VMEM((2, 12, 192), F32),
        pltpu.VMEM((8, 128), F32),
        pltpu.SemaphoreType.DMA((13,)),
        pltpu.SemaphoreType.DMA((12,)),
        pltpu.SemaphoreType.DMA((2,)),
    ]
    return pl.pallas_call(
        cell_kernel,
        out_shape=outs,
        in_specs=[ANYWHERE] * 14,
        out_specs=[WHOLE] * 5 + [ANYWHERE] * 2,
        scratch_shapes=scratch,
        name="cell",
        compiler_params=pltpu.CompilerParams(vmem_limit_bytes=24 * MIB),
    )(*(pltpu.with_memory_space_constraint(a, pltpu.HBM) for a in args))


def update_kernel(mem, wkey_t, value, keep, order, out, done, new_v, sem):
    done[...] = jnp.zeros((8, 128), F32)
    copies = []
    for b in range(12):
        for h in range(2):
            span = slice(h * 192, (h + 1) * 192)
            new_v[b, h] = (
                keep[h, b : b + 1, :] * mem[b, h] + wkey_t[span, b : b + 1] * value[h, b : b + 1, :]
            )
        cp = pltpu.make_async_copy(new_v.at[b], out.at[b], sem.at[b])
        cp.start()
        copies.append(cp)
    for cp in copies:
        cp.wait()


def update(mem, wkey_t, value, keep, order):
    return pl.pallas_call(
        update_kernel,
        out_shape=[jax.ShapeDtypeStruct(mem.shape, F32), pltpu.VMEM((8, 128), F32)],
        in_specs=[WHOLE] * 5,
        out_specs=[ANYWHERE, WHOLE],
        scratch_shapes=[pltpu.VMEM(mem.shape, F32), pltpu.SemaphoreType.DMA((12,))],
        name="update",
        compiler_params=pltpu.CompilerParams(vmem_limit_bytes=12 * MIB),
    )(near(mem), near(wkey_t), near(value), near(keep), near(order))


def load_kernel(gate, up, down, order, gate_v, up_v, down_v, done, sem):
    done[...] = jnp.zeros((8, 128), F32)
    copies = [
        pltpu.make_async_copy(src.at[0], dst, sem.at[i])
        for i, (src, dst) in enumerate(((gate, gate_v), (up, up_v), (down, down_v)))
    ]
    for cp in copies:
        cp.start()
    for cp in copies:
        cp.wait()


def load(gate, up, down, order):
    return pl.pallas_call(
        load_kernel,
        out_shape=[*(pltpu.VMEM(w.shape[1:], BF16) for w in (gate, up, down)), pltpu.VMEM((8, 128), F32)],
        in_specs=[ANYWHERE] * 3 + [WHOLE],
        out_specs=[WHOLE] * 4,
        scratch_shapes=[pltpu.SemaphoreType.DMA((3,))],
        name="load",
        compiler_params=pltpu.CompilerParams(vmem_limit_bytes=4 * MIB),
    )(*(pltpu.with_memory_space_constraint(w, pltpu.HBM) for w in (gate, up, down)), near(order))


def near(x):
    return pltpu.with_memory_space_constraint(x, pltpu.VMEM)


HALF, META = 1024, 1152
SIDE = Z * 24


def mix_kernel(tok, mine, other, gain, ids, probs, order, block_out, resid_out, scr):
    mixed = (mine[...].astype(F32) + other[...].astype(F32)).astype(BF16)
    resid = (tok[...].astype(F32) + mixed.astype(F32)).astype(BF16)
    resid_out[...] = resid
    x = resid.astype(F32)
    normed = x * lax.rsqrt(jnp.mean(x * x, axis=-1, keepdims=True) + EPS) * gain[...]
    weights = probs[...] / jnp.sum(probs[...], axis=0, keepdims=True)
    high = weights.astype(BF16)
    low = (weights - high.astype(F32)).astype(BF16)
    lane = lax.broadcasted_iota(jnp.int32, (4, 128), 1)
    row = lax.broadcasted_iota(jnp.int32, (4, 128), 0)
    meta = jnp.zeros((12, 128), F32)
    for i, v in enumerate(((ids[...] + 1).astype(F32).astype(BF16), high, low)):
        place = (lane == row + 4 * i).astype(F32).astype(BF16)
        meta = meta + lax.dot_general(v, place, (((0,), (0,)), ((), ())), preferred_element_type=F32)
    for h in range(2):
        scr[h * 12 : h * 12 + 12, 0:HALF] = normed[:, h * HALF : (h + 1) * HALF]
        scr[h * 12 : h * 12 + 12, HALF:META] = meta
    block = scr[...].astype(BF16)
    for j in range(Z):
        block_out[j] = block


def mix(tokens, mine, other, gain, ids, probs, order):
    return pl.pallas_call(
        mix_kernel,
        out_shape=[pltpu.VMEM((Z, 24, META), BF16), pltpu.VMEM((12, 2048), BF16)],
        in_specs=[WHOLE] * 7,
        out_specs=[WHOLE] * 2,
        scratch_shapes=[pltpu.VMEM((24, META), F32)],
        name="mix",
        compiler_params=pltpu.CompilerParams(vmem_limit_bytes=8 * MIB),
    )(near(tokens), near(mine), near(other), near(gain), near(ids), near(probs), near(order))


def choose(col, weights_out):
    z, y, xh, c = (lax.axis_index(a) for a in EP)
    row = lax.broadcasted_iota(jnp.int32, (128, SIDE), 0)
    lane = lax.broadcasted_iota(jnp.int32, (128, SIDE), 1)
    dy, dx = jnp.zeros_like(row), jnp.zeros_like(row)
    for j, (step_y, step_x) in enumerate(STEPS):
        dy = jnp.where((row >> 4) == j, step_y, dy)
        dx = jnp.where((row >> 4) == j, step_x, dx)
    expert = ((z * Y + ((y + dy) & 3)) * XH + (xh ^ dx)) * C + c + 1
    expert = expert.astype(F32)
    pick = (
        lax.broadcasted_iota(jnp.int32, (16, 128), 1) == lax.broadcasted_iota(jnp.int32, (16, 128), 0)
    ).astype(F32).astype(BF16)
    group = (lane * 171) >> 11
    origin = lax.broadcasted_iota(jnp.int32, (SIDE, SIDE), 0)
    target = lax.broadcasted_iota(jnp.int32, (SIDE, SIDE), 1)
    before = (((origin * 171) >> 11) == ((target * 171) >> 11)) & (origin < target)
    before = before.astype(F32).astype(BF16)
    same = ((row >> 1) & 7) == (group >> 1)
    slot = (row & 1).astype(F32)
    found = lax.dot_general(pick, col[:, HALF:META], (((1,), (1,)), ((), ())), preferred_element_type=F32)
    hit = jnp.zeros((128, SIDE), F32)
    w_high = jnp.zeros((128, SIDE), F32)
    w_low = jnp.zeros((128, SIDE), F32)
    for k in range(4):
        match = found[k : k + 1] == expert
        hit = hit + jnp.where(match, 1.0, 0.0)
        w_high = w_high + jnp.where(match, found[4 + k : 5 + k], 0.0)
        w_low = w_low + jnp.where(match, found[8 + k : 9 + k], 0.0)
    earlier = jnp.dot(hit.astype(BF16), before, preferred_element_type=F32)
    mask = same & (earlier == slot)
    chosen = []
    for h in range(2):
        part = mask & ((group & 1) == h)
        weights_out[h, 0] = jnp.where(part, w_high, 0.0).astype(BF16)
        weights_out[h, 1] = jnp.where(part, w_low, 0.0).astype(BF16)
        chosen.append(
            jnp.dot(
                jnp.where(part, hit, 0.0).astype(BF16), col[:, 0:HALF], preferred_element_type=F32
            ).astype(BF16)
        )
    return chosen


WEIGHTS = (2, 2, 128, SIDE)


def pack_own_kernel(col, chosen_out, weights_out):
    for h, chosen in enumerate(choose(col, weights_out)):
        chosen_out[:, h * HALF : (h + 1) * HALF] = chosen


def pack_own(col):
    return pl.pallas_call(
        pack_own_kernel,
        out_shape=[pltpu.VMEM((128, 2048), BF16), pltpu.VMEM(WEIGHTS, BF16)],
        in_specs=[WHOLE],
        out_specs=[WHOLE] * 2,
        name="pack_own",
        compiler_params=pltpu.CompilerParams(vmem_limit_bytes=12 * MIB),
    )(near(col))


def pack_kernel(col, own, *refs):
    sent, weights_out = refs[:8], refs[8]
    for j in range(8):
        sent[j][0:16, :] = own[j * 16 : (j + 1) * 16, :]
    for h, chosen in enumerate(choose(col, weights_out)):
        for j in range(8):
            sent[j][16:32, h * HALF : (h + 1) * HALF] = chosen[j * 16 : (j + 1) * 16]


def pack(col, own):
    return pl.pallas_call(
        pack_kernel,
        out_shape=[pltpu.VMEM((32, 2048), BF16)] * 8 + [pltpu.VMEM(WEIGHTS, BF16)],
        in_specs=[WHOLE] * 2,
        out_specs=[WHOLE] * 9,
        name="pack",
        compiler_params=pltpu.CompilerParams(vmem_limit_bytes=12 * MIB),
    )(near(col), near(own))


def combine_kernel(side, weights, order, *refs):
    back, out, scr = refs[:8], refs[8], refs[9]
    dims = (((0,), (0,)), ((), ()))
    for j in range(8):
        scr[j * 16 : (j + 1) * 16, :] = back[j][side * 16 : (side + 1) * 16, :]
    total = jnp.zeros((SIDE, HALF), F32)
    for h in range(2):
        values = scr[:, h * HALF : (h + 1) * HALF]
        for i in range(2):
            total = total + lax.dot_general(weights[h, i], values, dims, preferred_element_type=F32)
    out[...] = total.astype(out.dtype)


def combine(weights, order, back, side, dtype):
    return pl.pallas_call(
        functools.partial(combine_kernel, side),
        out_shape=pltpu.VMEM((SIDE, HALF), dtype),
        in_specs=[WHOLE] * 10,
        out_specs=WHOLE,
        scratch_shapes=[pltpu.VMEM((128, 2048), BF16)],
        name="combine",
        compiler_params=pltpu.CompilerParams(vmem_limit_bytes=12 * MIB),
    )(near(weights), near(order), *(near(b) for b in back))


def add_kernel(mine, other, out):
    out[...] = (mine[...] + other[...].astype(F32)).astype(BF16)


def add(mine, other):
    return pl.pallas_call(
        add_kernel,
        out_shape=pltpu.VMEM(mine.shape, BF16),
        in_specs=[WHOLE] * 2,
        out_specs=WHOLE,
        name="add",
        compiler_params=pltpu.CompilerParams(vmem_limit_bytes=8 * MIB),
    )(near(mine), near(other))


def gather_kernel(parts, total_out, sent_out):
    total = parts[0].astype(F32)
    for j in range(1, Z):
        total = total + parts[j].astype(F32)
    total_out[...] = total
    sent_out[...] = total.astype(BF16)


def gather(parts):
    return pl.pallas_call(
        gather_kernel,
        out_shape=[pltpu.VMEM((24, HALF), F32), pltpu.VMEM((24, HALF), BF16)],
        in_specs=[WHOLE],
        out_specs=[WHOLE] * 2,
        name="gather",
        compiler_params=pltpu.CompilerParams(vmem_limit_bytes=8 * MIB),
    )(near(parts))


def finish_kernel(resid, mine, other, out, scr):
    scr[...] = mine[...] + other[...].astype(F32)
    for h in range(2):
        cols = slice(h * HALF, (h + 1) * HALF)
        out[:, cols] = (resid[:, cols].astype(F32) + scr[h * 12 : h * 12 + 12, :]).astype(BF16)


def finish(resid, mine, other):
    return pl.pallas_call(
        finish_kernel,
        out_shape=jax.ShapeDtypeStruct((12, 2048), BF16),
        in_specs=[WHOLE] * 3,
        scratch_shapes=[pltpu.VMEM((24, HALF), F32)],
        name="finish",
        compiler_params=pltpu.CompilerParams(vmem_limit_bytes=8 * MIB),
    )(near(resid), near(mine), near(other))


def expert_kernel(*refs):
    rows, (gate, up, down), outs, x = refs[:4], refs[4:7], refs[7:11], refs[11]
    for j in range(4):
        x[j * 32 : (j + 1) * 32, :] = rows[j][...]
    gate_val = jnp.dot(x[...], gate[...], preferred_element_type=F32)
    up_val = jnp.dot(x[...], up[...], preferred_element_type=F32)
    hidden = (gate_val * jax.nn.sigmoid(gate_val) * up_val).astype(BF16)
    total = jnp.dot(hidden, down[...], preferred_element_type=F32)
    for j in range(4):
        outs[j][...] = total[j * 32 : (j + 1) * 32, :].astype(BF16)


def expert(rows, weights):
    return pl.pallas_call(
        expert_kernel,
        out_shape=[pltpu.VMEM((32, 2048), BF16)] * 4,
        in_specs=[WHOLE] * 7,
        out_specs=[WHOLE] * 4,
        scratch_shapes=[pltpu.VMEM((128, 2048), BF16)],
        name="expert",
        compiler_params=pltpu.CompilerParams(vmem_limit_bytes=16 * MIB),
    )(*(near(r) for r in rows), *(near(w) for w in weights))


def local(
    tokens,
    norm_gain,
    w_query,
    w_key,
    w_value,
    w_outgate,
    w_input_gate,
    w_forget_gate,
    forget_bias,
    head_gain,
    w_output,
    memory,
    normalizer,
    stabilizer,
    ffn_gain,
    route_ids,
    route_probs,
    expert_gate,
    expert_up,
    expert_down,
):
    partial_value, mem_near, wkey_t, value, keep, new_normalizer, new_stab = cell(
        tokens,
        norm_gain.reshape(1, -1),
        stabilizer.T,
        normalizer,
        forget_bias.reshape(1, -1),
        head_gain.reshape(6, 128),
        w_input_gate.T,
        w_forget_gate.T,
        w_query,
        w_key,
        w_value,
        w_outgate,
        w_output,
        memory,
    )
    other_value = lax.ppermute(partial_value, "tp", SWAP)
    *loaded, order = load(expert_gate, expert_up, expert_down, partial_value)
    blocks, resid = mix(
        tokens, partial_value, other_value, ffn_gain.reshape(1, -1), route_ids.T, route_probs.T, order
    )
    column = lax.all_to_all(blocks, "z", 0, 0, tiled=True).reshape(SIDE, META)
    column_other = lax.ppermute(column, "c", SWAP)
    own, weights_own = pack_own(column)
    *sent, weights_other = pack(column_other, own)
    incoming = plane_exchange(sent, False)
    outgoing = [*expert(incoming[:4], loaded), *expert(incoming[4:], loaded)]
    back = plane_exchange(outgoing, True)
    new_memory, order = update(mem_near, wkey_t, value, keep, outgoing[4])
    sum_b = lax.ppermute(combine(weights_other, order, back, 1, BF16), "c", SWAP)
    sum_a = combine(weights_own, order, back, 0, F32)
    sums = add(sum_a, sum_b).reshape(Z, 24, HALF)
    sums = lax.all_to_all(sums, "z", 0, 0, tiled=True)
    combined, sent_on = gather(sums)
    combined_other = lax.ppermute(sent_on, "tp", SWAP)
    next_tokens = finish(resid, combined, combined_other)
    return (next_tokens, new_memory, new_normalizer, new_stab.T)


def solution(mesh):
    fine = Mesh(mesh.devices.reshape(Z, Y, XH, C, TP), (*EP, "tp"))
    ep = EP
    return jax.shard_map(
        local,
        mesh=fine,
        in_specs=(
            P(ep, None),
            P(),
            P(None, "tp"),
            P(None, "tp"),
            P(None, "tp"),
            P(None, "tp"),
            P(),
            P(),
            P(),
            P(),
            P("tp", None),
            P(ep, "tp", None, None),
            P(ep, "tp", None),
            P(ep, "tp"),
            P(),
            P(ep, None),
            P(ep, None),
            P(ep, None, "tp"),
            P(ep, None, "tp"),
            P(ep, "tp", None),
        ),
        out_specs=(P(ep, None), P(ep, "tp", None, None), P(ep, "tp", None), P(ep, "tp")),
        check_vma=False,
    )
```

```python
import functools

import jax
import jax.numpy as jnp
from jax import lax
from jax.experimental import pallas as pl
from jax.experimental.pallas import tpu as pltpu
from jax.sharding import Mesh, PartitionSpec as P

EPS = 1e-06
Z, Y, XH, C, TP = 8, 4, 2, 2, 2
EP = ("z", "y", "xh", "c")
F32, BF16 = jnp.float32, jnp.bfloat16
MIB = 1 << 20


def plane_pairs(dy, dx, back):
    pairs = []
    for y in range(Y):
        for xh in range(XH):
            for t in range(TP):
                src = (y * XH + xh) * TP + t
                dst = (((y + dy) % Y) * XH + (xh ^ dx)) * TP + (t ^ dx)
                pairs.append((dst, src) if back else (src, dst))
    return pairs


STEPS = [(0, 0), (2, 0), (2, 1), (0, 1), (1, 0), (1, 1), (3, 0), (3, 1)]
BACK = [1, 2, 3, 5, 7, 4, 6]


def plane_exchange(parts, back):
    out = list(parts)
    for j in BACK if back else range(1, 8):
        out[j] = lax.ppermute(parts[j], ("y", "xh", "tp"), plane_pairs(*STEPS[j], back))
    return out


SWAP = [(0, 1), (1, 0)]


def cell_kernel(*refs):
    ins, outs, scr = refs[:14], refs[14:21], refs[21:]
    part_out, mem_v, wkey_out, value_out, keep_out, norm_hbm, stab_hbm = outs
    vm = scr[:13]
    norm_v, stab_v, num_v, gate_v, in_sem, mem_sem, out_sem = scr[13:]
    mem = ins[13]
    rows = 12
    copies = [pltpu.make_async_copy(ins[i], vm[i], in_sem.at[i]) for i in range(13)]
    mem_copies = [pltpu.make_async_copy(mem.at[b], mem_v.at[b], mem_sem.at[b]) for b in range(rows)]
    for i in range(12):
        copies[i].start()
    for cp in mem_copies:
        cp.start()
    copies[12].start()
    (tok, gain, stab, nrm, bias, hgain, wig, wfg, wq, wk, wv, wo, wout) = vm
    copies[0].wait()
    copies[1].wait()
    x = tok[...].astype(F32)
    normed = (x * lax.rsqrt(jnp.mean(x * x, axis=-1, keepdims=True) + EPS) * gain[...]).astype(BF16)
    for i in range(2, 8):
        copies[i].wait()
    first_half = lax.axis_index("tp") == 0

    def own(weights):
        both = lax.dot_general(weights[...], normed, (((1,), (1,)), ((), ())), preferred_element_type=F32)
        return jnp.where(first_half, both[0:2], both[2:4])

    input_pre = own(wig)
    biases = bias[...]
    column = lax.broadcasted_iota(jnp.int32, (2, rows), 0)
    low_bias = jnp.where(first_half, biases[:, 0:1], biases[:, 2:3])
    high_bias = jnp.where(first_half, biases[:, 1:2], biases[:, 3:4])
    forget = own(wfg) + jnp.where(column == 0, low_bias, high_bias)
    log_forget = jnp.minimum(forget, 0.0) - jnp.log1p(jnp.exp(-jnp.abs(forget)))
    carried = log_forget + stab[...]
    new_stab = jnp.maximum(carried, input_pre)
    stab_v[...] = new_stab
    stab_copy = pltpu.make_async_copy(stab_v, stab_hbm, out_sem.at[0])
    stab_copy.start()
    gate_v[...] = jnp.zeros((8, 128), F32)
    gate_v[0:2, 0:rows] = jnp.exp(carried - new_stab)
    gate_v[2:4, 0:rows] = jnp.exp(input_pre - new_stab)
    gate_v[4:6, 0:rows] = jnp.exp(-new_stab)
    gates = jnp.transpose(gate_v[...])[0:rows]
    keep, write, floor = gates[:, 0:2], gates[:, 2:4], gates[:, 4:6]
    cut = lambda v, h: v[:, h * 192 : (h + 1) * 192]
    keeps = [jnp.broadcast_to(keep[:, h : h + 1], (rows, 192)) for h in range(2)]

    def turned(values):
        return jnp.transpose(jnp.concatenate([values, jnp.zeros((128 - rows, 384), F32)], axis=0))

    copies[8].wait()
    query = jnp.dot(normed, wq[...], preferred_element_type=F32)
    query_t = turned(query)
    copies[9].wait()
    key = jnp.dot(normed, wk[...], preferred_element_type=F32) * 192 ** (-0.5)
    head = lax.broadcasted_iota(jnp.int32, (rows, 384), 1) >= 192
    wkey = jnp.where(head, write[:, 1:2], write[:, 0:1]) * key
    wkey_out[...] = turned(wkey)
    scales, mixes = [], []
    for h in range(2):
        keep_out[h] = keeps[h]
        new_norm = keeps[h] * nrm[:, h, :] + cut(wkey, h)
        norm_v[:, h, :] = new_norm
        den = jnp.sum(cut(query, h) * new_norm, axis=-1, keepdims=True)
        scales.append(jnp.maximum(jnp.abs(den), floor[:, h : h + 1]))
        mixes.append(jnp.sum(cut(query, h) * cut(wkey, h), axis=-1, keepdims=True))
    norm_copy = pltpu.make_async_copy(norm_v, norm_hbm, out_sem.at[1])
    norm_copy.start()
    copies[10].wait()
    value = jnp.dot(normed, wv[...], preferred_element_type=F32)
    copies[11].wait()
    outgate = jnp.dot(normed, wo[...], preferred_element_type=F32)
    gain_rows = jnp.where(first_half, hgain[0:3, :], hgain[3:6, :])
    gains = jnp.concatenate([gain_rows[i : i + 1] for i in range(3)], axis=1)
    own_values = [cut(value, h) for h in range(2)]
    shapes = [jax.nn.sigmoid(cut(outgate, h)) for h in range(2)]
    for h in range(2):
        value_out[h] = own_values[h]
    for b in range(rows):
        mem_copies[b].wait()
        for h in range(2):
            span = slice(h * 192, (h + 1) * 192)
            num_v[h, b : b + 1, :] = jnp.sum(query_t[span, b : b + 1] * mem_v[b, h], axis=0, keepdims=True)
    total = None
    copies[12].wait()
    for h in range(2):
        readout = (keeps[h] * num_v[h] + mixes[h] * own_values[h]) / scales[h]
        scaled = readout * lax.rsqrt(jnp.mean(readout * readout, axis=-1, keepdims=True) + EPS) * cut(gains, h)
        gated = (scaled * shapes[h]).astype(BF16)
        part = jnp.dot(gated, wout[h * 192 : (h + 1) * 192, :], preferred_element_type=F32)
        total = part if total is None else total + part
    part_out[...] = total.astype(BF16)
    stab_copy.wait()
    norm_copy.wait()


ANYWHERE = pl.BlockSpec(memory_space=pl.ANY)
WHOLE = pl.BlockSpec(memory_space=pltpu.VMEM)


def cell(*args):
    memory, nrm, stab = args[13], args[3], args[2]
    outs = [
        pltpu.VMEM((12, 2048), BF16),
        pltpu.VMEM(memory.shape, F32),
        pltpu.VMEM((384, 128), F32),
        pltpu.VMEM((2, 12, 192), F32),
        pltpu.VMEM((2, 12, 192), F32),
        jax.ShapeDtypeStruct(nrm.shape, F32),
        jax.ShapeDtypeStruct(stab.shape, F32),
    ]
    scratch = [pltpu.VMEM(a.shape, a.dtype) for a in args[:13]]
    scratch += [
        pltpu.VMEM(nrm.shape, F32),
        pltpu.VMEM(stab.shape, F32),
        pltpu.VMEM((2, 12, 192), F32),
        pltpu.VMEM((8, 128), F32),
        pltpu.SemaphoreType.DMA((13,)),
        pltpu.SemaphoreType.DMA((12,)),
        pltpu.SemaphoreType.DMA((2,)),
    ]
    return pl.pallas_call(
        cell_kernel,
        out_shape=outs,
        in_specs=[ANYWHERE] * 14,
        out_specs=[WHOLE] * 5 + [ANYWHERE] * 2,
        scratch_shapes=scratch,
        name="cell",
        compiler_params=pltpu.CompilerParams(vmem_limit_bytes=24 * MIB),
    )(*(pltpu.with_memory_space_constraint(a, pltpu.HBM) for a in args))


def update_kernel(mem, wkey_t, value, keep, order, out, done, new_v, sem):
    done[...] = jnp.zeros((8, 128), F32)
    copies = []
    for b in range(12):
        for h in range(2):
            span = slice(h * 192, (h + 1) * 192)
            new_v[b, h] = (
                keep[h, b : b + 1, :] * mem[b, h] + wkey_t[span, b : b + 1] * value[h, b : b + 1, :]
            )
        cp = pltpu.make_async_copy(new_v.at[b], out.at[b], sem.at[b])
        cp.start()
        copies.append(cp)
    for cp in copies:
        cp.wait()


def update(mem, wkey_t, value, keep, order):
    return pl.pallas_call(
        update_kernel,
        out_shape=[jax.ShapeDtypeStruct(mem.shape, F32), pltpu.VMEM((8, 128), F32)],
        in_specs=[WHOLE] * 5,
        out_specs=[ANYWHERE, WHOLE],
        scratch_shapes=[pltpu.VMEM(mem.shape, F32), pltpu.SemaphoreType.DMA((12,))],
        name="update",
        compiler_params=pltpu.CompilerParams(vmem_limit_bytes=12 * MIB),
    )(near(mem), near(wkey_t), near(value), near(keep), near(order))


def load_kernel(gate, up, down, order, gate_v, up_v, down_v, done, sem):
    done[...] = jnp.zeros((8, 128), F32)
    copies = [
        pltpu.make_async_copy(src.at[0], dst, sem.at[i])
        for i, (src, dst) in enumerate(((gate, gate_v), (up, up_v), (down, down_v)))
    ]
    for cp in copies:
        cp.start()
    for cp in copies:
        cp.wait()


def load(gate, up, down, order):
    return pl.pallas_call(
        load_kernel,
        out_shape=[*(pltpu.VMEM(w.shape[1:], BF16) for w in (gate, up, down)), pltpu.VMEM((8, 128), F32)],
        in_specs=[ANYWHERE] * 3 + [WHOLE],
        out_specs=[WHOLE] * 4,
        scratch_shapes=[pltpu.SemaphoreType.DMA((3,))],
        name="load",
        compiler_params=pltpu.CompilerParams(vmem_limit_bytes=4 * MIB),
    )(*(pltpu.with_memory_space_constraint(w, pltpu.HBM) for w in (gate, up, down)), near(order))


def near(x):
    return pltpu.with_memory_space_constraint(x, pltpu.VMEM)


HALF, META = 1024, 1152
SIDE = Z * 24


def mix_kernel(tok, mine, other, gain, ids, probs, order, block_out, resid_out, scr):
    mixed = (mine[...].astype(F32) + other[...].astype(F32)).astype(BF16)
    resid = (tok[...].astype(F32) + mixed.astype(F32)).astype(BF16)
    resid_out[...] = resid
    x = resid.astype(F32)
    normed = x * lax.rsqrt(jnp.mean(x * x, axis=-1, keepdims=True) + EPS) * gain[...]
    weights = probs[...] / jnp.sum(probs[...], axis=0, keepdims=True)
    high = weights.astype(BF16)
    low = (weights - high.astype(F32)).astype(BF16)
    lane = lax.broadcasted_iota(jnp.int32, (4, 128), 1)
    row = lax.broadcasted_iota(jnp.int32, (4, 128), 0)
    meta = jnp.zeros((12, 128), F32)
    for i, v in enumerate(((ids[...] + 1).astype(F32).astype(BF16), high, low)):
        place = (lane == row + 4 * i).astype(F32).astype(BF16)
        meta = meta + lax.dot_general(v, place, (((0,), (0,)), ((), ())), preferred_element_type=F32)
    for h in range(2):
        scr[h * 12 : h * 12 + 12, 0:HALF] = normed[:, h * HALF : (h + 1) * HALF]
        scr[h * 12 : h * 12 + 12, HALF:META] = meta
    block = scr[...].astype(BF16)
    for j in range(Z):
        block_out[j] = block


def mix(tokens, mine, other, gain, ids, probs, order):
    return pl.pallas_call(
        mix_kernel,
        out_shape=[pltpu.VMEM((Z, 24, META), BF16), pltpu.VMEM((12, 2048), BF16)],
        in_specs=[WHOLE] * 7,
        out_specs=[WHOLE] * 2,
        scratch_shapes=[pltpu.VMEM((24, META), F32)],
        name="mix",
        compiler_params=pltpu.CompilerParams(vmem_limit_bytes=8 * MIB),
    )(near(tokens), near(mine), near(other), near(gain), near(ids), near(probs), near(order))


def choose(col, weights_out):
    z, y, xh, c = (lax.axis_index(a) for a in EP)
    row = lax.broadcasted_iota(jnp.int32, (128, SIDE), 0)
    lane = lax.broadcasted_iota(jnp.int32, (128, SIDE), 1)
    dy, dx = jnp.zeros_like(row), jnp.zeros_like(row)
    for j, (step_y, step_x) in enumerate(STEPS):
        dy = jnp.where((row >> 4) == j, step_y, dy)
        dx = jnp.where((row >> 4) == j, step_x, dx)
    expert = ((z * Y + ((y + dy) & 3)) * XH + (xh ^ dx)) * C + c + 1
    expert = expert.astype(F32)
    pick = (
        lax.broadcasted_iota(jnp.int32, (16, 128), 1) == lax.broadcasted_iota(jnp.int32, (16, 128), 0)
    ).astype(F32).astype(BF16)
    group = (lane * 171) >> 11
    origin = lax.broadcasted_iota(jnp.int32, (SIDE, SIDE), 0)
    target = lax.broadcasted_iota(jnp.int32, (SIDE, SIDE), 1)
    before = (((origin * 171) >> 11) == ((target * 171) >> 11)) & (origin < target)
    before = before.astype(F32).astype(BF16)
    same = ((row >> 1) & 7) == (group >> 1)
    slot = (row & 1).astype(F32)
    found = lax.dot_general(pick, col[:, HALF:META], (((1,), (1,)), ((), ())), preferred_element_type=F32)
    hit = jnp.zeros((128, SIDE), F32)
    w_high = jnp.zeros((128, SIDE), F32)
    w_low = jnp.zeros((128, SIDE), F32)
    for k in range(4):
        match = found[k : k + 1] == expert
        hit = hit + jnp.where(match, 1.0, 0.0)
        w_high = w_high + jnp.where(match, found[4 + k : 5 + k], 0.0)
        w_low = w_low + jnp.where(match, found[8 + k : 9 + k], 0.0)
    earlier = jnp.dot(hit.astype(BF16), before, preferred_element_type=F32)
    mask = same & (earlier == slot)
    chosen = []
    for h in range(2):
        part = mask & ((group & 1) == h)
        weights_out[h, 0] = jnp.where(part, w_high, 0.0).astype(BF16)
        weights_out[h, 1] = jnp.where(part, w_low, 0.0).astype(BF16)
        chosen.append(
            jnp.dot(
                jnp.where(part, hit, 0.0).astype(BF16), col[:, 0:HALF], preferred_element_type=F32
            ).astype(BF16)
        )
    return chosen


WEIGHTS = (2, 2, 128, SIDE)


def pack_own_kernel(col, chosen_out, weights_out):
    for h, chosen in enumerate(choose(col, weights_out)):
        chosen_out[:, h * HALF : (h + 1) * HALF] = chosen


def pack_own(col):
    return pl.pallas_call(
        pack_own_kernel,
        out_shape=[pltpu.VMEM((128, 2048), BF16), pltpu.VMEM(WEIGHTS, BF16)],
        in_specs=[WHOLE],
        out_specs=[WHOLE] * 2,
        name="pack_own",
        compiler_params=pltpu.CompilerParams(vmem_limit_bytes=12 * MIB),
    )(near(col))


def pack_kernel(col, own, *refs):
    sent, weights_out = refs[:8], refs[8]
    for j in range(8):
        sent[j][0:16, :] = own[j * 16 : (j + 1) * 16, :]
    for h, chosen in enumerate(choose(col, weights_out)):
        for j in range(8):
            sent[j][16:32, h * HALF : (h + 1) * HALF] = chosen[j * 16 : (j + 1) * 16]


def pack(col, own):
    return pl.pallas_call(
        pack_kernel,
        out_shape=[pltpu.VMEM((32, 2048), BF16)] * 8 + [pltpu.VMEM(WEIGHTS, BF16)],
        in_specs=[WHOLE] * 2,
        out_specs=[WHOLE] * 9,
        name="pack",
        compiler_params=pltpu.CompilerParams(vmem_limit_bytes=12 * MIB),
    )(near(col), near(own))


def combine_kernel(side, weights, order, *refs):
    back, out, scr = refs[:8], refs[8], refs[9]
    dims = (((0,), (0,)), ((), ()))
    for j in range(8):
        scr[j * 16 : (j + 1) * 16, :] = back[j][side * 16 : (side + 1) * 16, :]
    total = jnp.zeros((SIDE, HALF), F32)
    for h in range(2):
        values = scr[:, h * HALF : (h + 1) * HALF]
        for i in range(2):
            total = total + lax.dot_general(weights[h, i], values, dims, preferred_element_type=F32)
    out[...] = total.astype(out.dtype)


def combine(weights, order, back, side, dtype):
    return pl.pallas_call(
        functools.partial(combine_kernel, side),
        out_shape=pltpu.VMEM((SIDE, HALF), dtype),
        in_specs=[WHOLE] * 10,
        out_specs=WHOLE,
        scratch_shapes=[pltpu.VMEM((128, 2048), BF16)],
        name="combine",
        compiler_params=pltpu.CompilerParams(vmem_limit_bytes=12 * MIB),
    )(near(weights), near(order), *(near(b) for b in back))


def add_kernel(mine, other, out):
    out[...] = (mine[...] + other[...].astype(F32)).astype(BF16)


def add(mine, other):
    return pl.pallas_call(
        add_kernel,
        out_shape=pltpu.VMEM(mine.shape, BF16),
        in_specs=[WHOLE] * 2,
        out_specs=WHOLE,
        name="add",
        compiler_params=pltpu.CompilerParams(vmem_limit_bytes=8 * MIB),
    )(near(mine), near(other))


def gather_kernel(parts, total_out, sent_out):
    total = parts[0].astype(F32)
    for j in range(1, Z):
        total = total + parts[j].astype(F32)
    total_out[...] = total
    sent_out[...] = total.astype(BF16)


def gather(parts):
    return pl.pallas_call(
        gather_kernel,
        out_shape=[pltpu.VMEM((24, HALF), F32), pltpu.VMEM((24, HALF), BF16)],
        in_specs=[WHOLE],
        out_specs=[WHOLE] * 2,
        name="gather",
        compiler_params=pltpu.CompilerParams(vmem_limit_bytes=8 * MIB),
    )(near(parts))


def finish_kernel(resid, mine, other, out, scr):
    scr[...] = mine[...] + other[...].astype(F32)
    for h in range(2):
        cols = slice(h * HALF, (h + 1) * HALF)
        out[:, cols] = (resid[:, cols].astype(F32) + scr[h * 12 : h * 12 + 12, :]).astype(BF16)


def finish(resid, mine, other):
    return pl.pallas_call(
        finish_kernel,
        out_shape=jax.ShapeDtypeStruct((12, 2048), BF16),
        in_specs=[WHOLE] * 3,
        scratch_shapes=[pltpu.VMEM((24, HALF), F32)],
        name="finish",
        compiler_params=pltpu.CompilerParams(vmem_limit_bytes=8 * MIB),
    )(near(resid), near(mine), near(other))


def expert_kernel(*refs):
    rows, (gate, up, down), outs, x = refs[:4], refs[4:7], refs[7:11], refs[11]
    for j in range(4):
        x[j * 32 : (j + 1) * 32, :] = rows[j][...]
    gate_val = jnp.dot(x[...], gate[...], preferred_element_type=F32)
    up_val = jnp.dot(x[...], up[...], preferred_element_type=F32)
    hidden = (gate_val * jax.nn.sigmoid(gate_val) * up_val).astype(BF16)
    total = jnp.dot(hidden, down[...], preferred_element_type=F32)
    for j in range(4):
        outs[j][...] = total[j * 32 : (j + 1) * 32, :].astype(BF16)


def expert(rows, weights):
    return pl.pallas_call(
        expert_kernel,
        out_shape=[pltpu.VMEM((32, 2048), BF16)] * 4,
        in_specs=[WHOLE] * 7,
        out_specs=[WHOLE] * 4,
        scratch_shapes=[pltpu.VMEM((128, 2048), BF16)],
        name="expert",
        compiler_params=pltpu.CompilerParams(vmem_limit_bytes=16 * MIB),
    )(*(near(r) for r in rows), *(near(w) for w in weights))


def local(
    tokens,
    norm_gain,
    w_query,
    w_key,
    w_value,
    w_outgate,
    w_input_gate,
    w_forget_gate,
    forget_bias,
    head_gain,
    w_output,
    memory,
    normalizer,
    stabilizer,
    ffn_gain,
    route_ids,
    route_probs,
    expert_gate,
    expert_up,
    expert_down,
):
    partial_value, mem_near, wkey_t, value, keep, new_normalizer, new_stab = cell(
        tokens,
        norm_gain.reshape(1, -1),
        stabilizer.T,
        normalizer,
        forget_bias.reshape(1, -1),
        head_gain.reshape(6, 128),
        w_input_gate.T,
        w_forget_gate.T,
        w_query,
        w_key,
        w_value,
        w_outgate,
        w_output,
        memory,
    )
    other_value = lax.ppermute(partial_value, "tp", SWAP)
    *loaded, order = load(expert_gate, expert_up, expert_down, partial_value)
    blocks, resid = mix(
        tokens, partial_value, other_value, ffn_gain.reshape(1, -1), route_ids.T, route_probs.T, order
    )
    column = lax.all_to_all(blocks, "z", 0, 0, tiled=True).reshape(SIDE, META)
    column_other = lax.ppermute(column, "c", SWAP)
    own, weights_own = pack_own(column)
    *sent, weights_other = pack(column_other, own)
    incoming = plane_exchange(sent, False)
    outgoing = [*expert(incoming[:4], loaded), *expert(incoming[4:], loaded)]
    back = plane_exchange(outgoing, True)
    new_memory, order = update(mem_near, wkey_t, value, keep, outgoing[4])
    sum_b = lax.ppermute(combine(weights_other, order, back, 1, BF16), "c", SWAP)
    sum_a = combine(weights_own, order, back, 0, F32)
    sums = add(sum_a, sum_b).reshape(Z, 24, HALF)
    sums = lax.all_to_all(sums, "z", 0, 0, tiled=True)
    combined, sent_on = gather(sums)
    combined_other = lax.ppermute(sent_on, "tp", SWAP)
    next_tokens = finish(resid, combined, combined_other)
    return (next_tokens, new_memory, new_normalizer, new_stab.T)


def solution(mesh):
    fine = Mesh(mesh.devices.reshape(Z, Y, XH, C, TP), (*EP, "tp"))
    ep = EP
    return jax.shard_map(
        local,
        mesh=fine,
        in_specs=(
            P(ep, None),
            P(),
            P(None, "tp"),
            P(None, "tp"),
            P(None, "tp"),
            P(None, "tp"),
            P(),
            P(),
            P(),
            P(),
            P("tp", None),
            P(ep, "tp", None, None),
            P(ep, "tp", None),
            P(ep, "tp"),
            P(),
            P(ep, None),
            P(ep, None),
            P(ep, None, "tp"),
            P(ep, None, "tp"),
            P(ep, "tp", None),
        ),
        out_specs=(P(ep, None), P(ep, "tp", None, None), P(ep, "tp", None), P(ep, "tp")),
        check_vma=False,
    )
```
